32 devices in a mesh: ep: 8 (over z, y), tp: 4 (over x, core).
Axes of the slice: x: 2, y: 2, z: 4, core: 2. Of those that a mesh axis runs over, the one named last changes fastest.
Arguments:
- hidden_in: bfloat16 [384, 2048], P('ep'), may hold values from -6 to 6
- carried_state: float32 [384, 4, 128, 256], P('ep', 'tp'), may hold values from -6 to 6
- input_gain: bfloat16 [2048], replicated, may hold values from 0.099609375 to 1.8984375
- query_weight: bfloat16 [2048, 512], P(None, 'tp'), may hold values from -0.125 to 0.125
- key_weight: bfloat16 [2048, 512], P(None, 'tp'), may hold values from -0.125 to 0.125
- value_weight: bfloat16 [2048, 1024], P(None, 'tp'), may hold values from -0.125 to 0.125
- outgate_weight: bfloat16 [2048, 1024], P(None, 'tp'), may hold values from -0.125 to 0.125
- decay_weight: bfloat16 [2048, 512], P(None, 'tp'), may hold values from -0.5 to 0.5
- decay_shift: float32 [384, 512], P('ep', 'tp'), may hold values from -0.7 to 0
- head_gain: bfloat16 [4, 256], P('tp'), may hold values from 0.099609375 to 1.8984375
- output_weight: bfloat16 [1024, 2048], P('tp'), may hold values from -0.1875 to 0.1875
- channel_gain: bfloat16 [2048], replicated, may hold values from 0.099609375 to 1.8984375
- branch_gate: bfloat16 [2048], replicated, may hold values from -0.125 to 0.125
- routes: int32 [384, 2], P('ep'), may hold values from 0 to 7, all different within a row; in each aligned block of 48 rows (0 to 47, 48 to 95, ...) at most 14 rows name the same one
- route_weights: float32 [384, 2], P('ep'), may hold values from 0.1 to 1
- expert_gate: bfloat16 [8, 2048, 3072], P('ep', None, 'tp'), may hold values from -0.125 to 0.125
- expert_up: bfloat16 [8, 2048, 3072], P('ep', None, 'tp'), may hold values from -0.125 to 0.125
- expert_down: bfloat16 [8, 3072, 2048], P('ep', 'tp'), may hold values from -0.109375 to 0.109375
- dense_gate: bfloat16 [2048, 4096], P('tp', 'ep'), may hold values from -0.125 to 0.125
- dense_up: bfloat16 [2048, 4096], P('tp', 'ep'), may hold values from -0.125 to 0.125
- dense_down: bfloat16 [4096, 2048], P('ep', 'tp'), may hold values from -0.09375 to 0.09375
Outputs:
- mixed: bfloat16 [384, 2048], P('ep', 'tp')
- new_state: float32 [384, 4, 128, 256], P('ep', 'tp')
The draws below stay inside these ranges and needn't reach their ends.
Inputs may be any that keep to these rules, and one draw needn't show every extreme that they name: `routes`: each row names 2 different experts. Among the rows of one index of ep no expert is named more than 14 times, and in every draw some expert is named exactly 14 times by the rows of some index.
All inputs are finite; a program needn't handle non-finite values.
Results may differ from the reference program's by a relative error of at most 0.02.
Values may be sent and summed in bfloat16 or wider, within the bound.
A program may use at most 128 MiB of HBM per device.

```python
import math
import jax
import jax.numpy as jnp
import numpy as np
from jax import lax

D = 2048
HEADS = 4
DK = 128
DV = 256
FF = 3072
DFF = 4096
TOPK = 2
SEQ_DEV = 48
BATCH = 384
EXPERTS = 8
CAP = 14
N_EP = 8
N_TP = 4


def level_of(stream_key, dims, pieces, smallest, largest):
    gain = 1.0
    for axis_at, blocks in pieces:
        draws = jax.random.uniform(jax.random.fold_in(jax.random.fold_in(stream_key, 6), axis_at), (blocks,), jnp.float32, smallest / len(pieces), largest / len(pieces))
        gain = gain * jnp.repeat(jnp.exp(draws), dims[axis_at] // blocks).reshape((-1,) + (1,) * (len(dims) - 1 - axis_at))
    return gain


def shared_out(key, own, number, rows, amount, top, limit, skew):
    ranking = jax.random.permutation(key, amount)
    crowded, common = shares(amount, rows * top, limit, skew, True), shares(amount, rows * top, limit, skew, False)
    places = jnp.arange(amount)

    def named(tallies, offset_by):
        used = int((tallies > 0).sum())
        fixed = max(1, used // 4)
        passed = fixed + (places - fixed + offset_by * (used - fixed)) % max(1, amount - fixed)
        return jnp.zeros((amount,), jnp.int32).at[ranking[jnp.where(places < fixed, places, passed)]].set(jnp.asarray(tallies, jnp.int32))

    tallies = jnp.where(number % 4 == 0, named(crowded, number // 4), named(common, number - number // 4 - 1))
    mixed = jax.random.permutation(jax.random.fold_in(own, 3), amount)
    donor, taker = mixed[0:amount // 2 * 2:2], mixed[1:amount // 2 * 2:2]
    slack = jnp.minimum(tallies[donor] - 1, limit - tallies[taker]) // 2
    slack = jnp.where((donor == ranking[0]) | (taker == ranking[0]) | (tallies[taker] == 0), 0, jnp.maximum(slack, 0))
    passed = jax.random.randint(jax.random.fold_in(own, 4), (amount // 2,), 0, 1 << 20) % (slack + 1)
    tallies = tallies.at[donor].add(-passed).at[taker].add(passed)
    members = jnp.searchsorted(jnp.cumsum(tallies), jnp.arange(rows * top), side="right").astype(jnp.int32)
    table = members.reshape(top, rows).T
    table = table[jax.random.permutation(jax.random.fold_in(own, 1), rows)]
    offset_by = jax.random.randint(jax.random.fold_in(own, 2), (rows, 1), 0, top)
    return jnp.take_along_axis(table, (jnp.arange(top)[None, :] + offset_by) % top, axis=1)


def shares(count, total, reach, slope, full):
    loads = [(1 << 20) // math.isqrt(standing ** slope) + 1 for standing in range(1, count + 1)]
    largest = reach if full else min(reach, max(-(-total // count), total * loads[0] // sum(loads)))
    least = 1 if total - largest >= count - 1 else 0
    counts, spare = [largest] + [least] * (count - 1), total - largest - least * (count - 1)
    while spare > 0:
        movable = [i for i in range(1, count) if counts[i] < largest] or [i for i in range(1, count) if counts[i] < reach]
        pool, remaining = sum([loads[i] for i in movable]), spare
        for i in movable:
            extra = min(reach - counts[i], max(1, remaining * loads[i] // pool), spare)
            counts[i] = counts[i] + extra
            spare = spare - extra
    return np.array(counts)


def gaussian(rng, dims, deviation, most, shards=(), held_as=jnp.bfloat16):
    values = deviation * jax.random.normal(rng, dims, jnp.float32)
    if shards:
        values = values * level_of(rng, dims, shards, -0.22, 0.18)
    return jnp.clip(values, -most, most).astype(held_as)


def setup_inputs(seed: int = 0) -> dict:
    streams_of = jax.random.split(jax.random.key(seed), 22)
    hidden_in = gaussian(streams_of[0], (BATCH, D), 1.0, 6.0, ((0, 8),))
    carried_state = gaussian(streams_of[1], (BATCH, HEADS, DK, DV), 1.0, 6.0, ((0, 8), (1, 4)), jnp.float32)
    input_gain = jnp.clip(1.0 + 0.18 * jax.random.normal(streams_of[2], (D,), jnp.float32), 0.099609375, 1.8984375).astype(jnp.bfloat16)
    query_weight = gaussian(streams_of[3], (D, HEADS * DK), D ** -0.5, 0.125, ((1, 4),))
    key_weight = gaussian(streams_of[4], (D, HEADS * DK), D ** -0.5, 0.125, ((1, 4),))
    value_weight = gaussian(streams_of[5], (D, HEADS * DV), D ** -0.5, 0.125, ((1, 4),))
    outgate_weight = gaussian(streams_of[6], (D, HEADS * DV), D ** -0.5, 0.125, ((1, 4),))
    decay_weight = gaussian(streams_of[7], (D, HEADS * DK), (D // 16) ** -0.5, 0.5, ((1, 4),))
    decay_shift = jnp.clip(-0.7 + 0.7 * jax.random.uniform(streams_of[8], (BATCH, HEADS * DK), jnp.float32) ** level_of(streams_of[8], (BATCH, HEADS * DK), ((0, 8), (1, 4)), -0.2, 0.2), -0.7, 0.0)
    head_gain = jnp.clip(1.0 + 0.18 * jax.random.normal(streams_of[9], (HEADS, DV), jnp.float32), 0.099609375, 1.8984375).astype(jnp.bfloat16)
    output_weight = gaussian(streams_of[10], (HEADS * DV, D), (HEADS * DV) ** -0.5, 0.1875, ((0, 4),))
    channel_gain = jnp.clip(1.0 + 0.18 * jax.random.normal(streams_of[11], (D,), jnp.float32), 0.099609375, 1.8984375).astype(jnp.bfloat16)
    branch_gate = gaussian(streams_of[12], (D,), D ** -0.5, 0.125)
    routes_keys = jax.random.split(jax.random.fold_in(streams_of[13], 1), BATCH // SEQ_DEV)
    routes_turns = jax.random.permutation(jax.random.fold_in(streams_of[13], 3), BATCH // SEQ_DEV)
    routes = jax.vmap(lambda own, number: shared_out(jax.random.fold_in(streams_of[13], 2), own, number, SEQ_DEV, EXPERTS, TOPK, CAP, 2))(routes_keys, routes_turns).reshape((BATCH, TOPK))
    route_weights = jnp.clip(0.1 + 0.9 * jax.random.uniform(streams_of[14], (BATCH, TOPK), jnp.float32) ** level_of(streams_of[14], (BATCH, TOPK), ((0, 8),), -0.2, 0.2), 0.1, 1.0)
    expert_gate = gaussian(streams_of[15], (EXPERTS, D, FF), D ** -0.5, 0.125, ((0, 8), (2, 4)))
    expert_up = gaussian(streams_of[16], (EXPERTS, D, FF), D ** -0.5, 0.125, ((0, 8), (2, 4)))
    expert_down = gaussian(streams_of[17], (EXPERTS, FF, D), FF ** -0.5, 0.109375, ((0, 8), (1, 4)))
    dense_gate = gaussian(streams_of[18], (D, DFF), D ** -0.5, 0.125, ((0, 4), (1, 8)))
    dense_up = gaussian(streams_of[19], (D, DFF), D ** -0.5, 0.125, ((0, 4), (1, 8)))
    dense_down = gaussian(streams_of[20], (DFF, D), DFF ** -0.5, 0.09375, ((0, 8), (1, 4)))
    return dict(hidden_in=hidden_in, carried_state=carried_state, input_gain=input_gain, query_weight=query_weight, key_weight=key_weight, value_weight=value_weight, outgate_weight=outgate_weight, decay_weight=decay_weight, decay_shift=decay_shift, head_gain=head_gain, output_weight=output_weight, channel_gain=channel_gain, branch_gate=branch_gate, routes=routes, route_weights=route_weights, expert_gate=expert_gate, expert_up=expert_up, expert_down=expert_down, dense_gate=dense_gate, dense_up=dense_up, dense_down=dense_down)


EPSILON = 1e-06
TAU_DECAY = 16.0

def rms_factor(values):
    return lax.rsqrt(lax.optimization_barrier(jnp.mean(values * values, axis=-1, keepdims=True)) + EPSILON)

def rounded(values):
    return lax.optimization_barrier(values.astype(jnp.bfloat16)).astype(jnp.float32)

def matmul(left, right):
    return jnp.dot(left, right, preferred_element_type=jnp.float32)

def expert_apply(token_rows, gate_matrix, up_matrix, down_matrix):
    block_width = gate_matrix.shape[1] // N_TP
    total = jnp.zeros((token_rows.shape[0], down_matrix.shape[1]), jnp.float32)
    for block in range(N_TP):
        lower = block * block_width
        gate_part = matmul(token_rows, gate_matrix[:, lower:lower + block_width])
        up_part = matmul(token_rows, up_matrix[:, lower:lower + block_width])
        hidden = (jax.nn.silu(gate_part) * up_part).astype(jnp.bfloat16)
        total = total + rounded(matmul(hidden, down_matrix[lower:lower + block_width]))
    return total

def reference(hidden_in, carried_state, input_gain, query_weight, key_weight, value_weight, outgate_weight, decay_weight, decay_shift, head_gain, output_weight, channel_gain, branch_gate, routes, route_weights, expert_gate, expert_up, expert_down, dense_gate, dense_up, dense_down):
    batch_size, width = hidden_in.shape
    head_count, key_dim, value_dim = carried_state.shape[1:]
    inputs = hidden_in.astype(jnp.float32)
    normed = (inputs * rms_factor(inputs) * input_gain.astype(jnp.float32)).astype(jnp.bfloat16)
    query = matmul(normed, query_weight).astype(jnp.bfloat16)
    key_rows = matmul(normed, key_weight).astype(jnp.bfloat16)
    value_rows = matmul(normed, value_weight).astype(jnp.bfloat16)
    outgate = matmul(normed, outgate_weight).astype(jnp.bfloat16)
    decay = jnp.exp(jax.nn.log_sigmoid(matmul(normed, decay_weight)) / TAU_DECAY + decay_shift)
    decay = decay.reshape(batch_size, head_count, key_dim)
    query_scaled = query.astype(jnp.float32).reshape(batch_size, head_count, key_dim) * key_dim ** (-0.5)
    key_vals = key_rows.astype(jnp.float32).reshape(batch_size, head_count, key_dim)
    value_vals = value_rows.astype(jnp.float32).reshape(batch_size, head_count, value_dim)
    new_state = decay[..., None] * carried_state + key_vals[..., None] * value_vals[:, :, None, :]
    readout = jnp.einsum('bhk,bhkv->bhv', query_scaled, new_state, precision=lax.Precision.HIGHEST)
    gate_vals = jax.nn.silu(outgate.astype(jnp.float32).reshape(batch_size, head_count, value_dim))
    gated = (readout * rms_factor(readout) * head_gain.astype(jnp.float32) * gate_vals).astype(jnp.bfloat16)
    group = head_count // N_TP
    attended = jnp.zeros((batch_size, width), jnp.float32)
    for block in range(N_TP):
        head_rows = gated[:, block * group:(block + 1) * group].reshape(batch_size, group * value_dim)
        weight_rows = output_weight[block * group * value_dim:(block + 1) * group * value_dim]
        attended = attended + rounded(matmul(head_rows, weight_rows))
    middle = rounded(inputs + attended)
    scaled = middle * rms_factor(middle) * channel_gain.astype(jnp.float32)
    branch = jax.nn.sigmoid(lax.optimization_barrier(jnp.sum(scaled * branch_gate.astype(jnp.float32), axis=-1)))
    ffn_in = scaled.astype(jnp.bfloat16)
    dense_hidden = (jax.nn.silu(matmul(ffn_in, dense_gate)) * matmul(ffn_in, dense_up)).astype(jnp.bfloat16)
    dense = matmul(dense_hidden, dense_down)
    topk = routes.shape[1]
    flat_routes = routes.reshape(-1)
    flat_tokens = (jnp.arange(flat_routes.shape[0], dtype=jnp.int32) // topk).astype(jnp.int32)
    flat_weights = route_weights.reshape(-1)
    capacity = N_EP * CAP

    def one_expert(carry, index):
        order = jnp.argsort((flat_routes != index).astype(jnp.int32), stable=True)[:capacity]
        valid = flat_routes[order] == index
        token_ids = flat_tokens[order]
        result = expert_apply(ffn_in[token_ids], expert_gate[index], expert_up[index], expert_down[index])
        weights = jnp.where(valid, flat_weights[order], jnp.zeros_like(flat_weights[order]))
        return (carry.at[token_ids].add(weights[:, None] * result), None)
    routed, _ = lax.scan(one_expert, jnp.zeros((batch_size, width), jnp.float32), jnp.arange(expert_gate.shape[0], dtype=jnp.int32))
    mixed = (middle + branch[:, None] * dense + routed).astype(jnp.bfloat16)
    return (mixed, new_state)
```

```python
import functools

import jax
import jax.numpy as jnp
from jax import lax
from jax.experimental import pallas as pl
from jax.experimental.pallas import tpu as pltpu
from jax.sharding import PartitionSpec as P

EPSILON = 1e-06
TAU_DECAY = 16.0
MESH = pl.DeviceIdType.MESH


def rms_factor(values):
    return lax.rsqrt(jnp.mean(values * values, axis=-1, keepdims=True) + EPSILON)


def matmul(left, right):
    return jnp.dot(left, right, preferred_element_type=jnp.float32)


def flat_row(ref):
    rows = ref[...].astype(jnp.float32)
    return jnp.concatenate([rows[k : k + 1, :] for k in range(rows.shape[0])], axis=1)


def silu(values):
    return values * jax.nn.sigmoid(values)


def layer_kernel(
    n_ep,
    n_tp,
    gated_ref,
    outw_ref,
    hid_ref,
    gain_ref,
    gate_ref,
    sel_ref,
    comb_hi_ref,
    comb_lo_ref,
    eg_hbm,
    eu_hbm,
    ed_hbm,
    dg_hbm,
    du_hbm,
    dd_hbm,
    mixed_ref,
    eg,
    eu,
    ed,
    dgw,
    duw,
    ddw,
    sel_recv,
    p_send,
    p_recv,
    st_send,
    st_recv,
    mid_buf,
    br_buf,
    piece,
    rows_all,
    g_send,
    g_recv,
    u_send,
    u_recv,
    e_hid,
    eo_send,
    eo_recv,
    d_hid,
    out_send,
    out_recv,
    ret_send,
    ret,
    w_sem,
    tp_ssem,
    tp_rsem,
    ep_ssem,
    ep_rsem,
    gain_row,
    gate_row,
):
    f32, bf16 = jnp.float32, jnp.bfloat16
    ep = lax.axis_index("ep")
    tp = lax.axis_index("tp")
    tokens, width = hid_ref.shape
    quarter = width // n_tp
    own = pl.ds(pl.multiple_of(tp * quarter, quarter), quarter)
    cap = sel_ref.shape[1]

    loads = []
    for i, (src, dst) in enumerate(
        ((dg_hbm, dgw), (du_hbm, duw), (eg_hbm, eg), (eu_hbm, eu), (ed_hbm, ed), (dd_hbm, ddw))
    ):
        load = pltpu.make_async_copy(src, dst, w_sem.at[i])
        load.start()
        loads.append(load)

    gain_row[...] = flat_row(gain_ref)
    gate_row[...] = flat_row(gate_ref)
    barrier = pltpu.get_barrier_semaphore()
    for d in range(1, n_tp):
        pl.semaphore_signal(
            barrier, inc=1, device_id=(ep, lax.rem(tp + d, n_tp)), device_id_type=MESH
        )
    for d in range(1, n_ep):
        pl.semaphore_signal(
            barrier, inc=1, device_id=(lax.rem(ep + d, n_ep), tp), device_id_type=MESH
        )

    def over_tp(phase, src_of, dst_of):
        copies = []
        for d in range(1, n_tp):
            peer = lax.rem(tp + d, n_tp)
            copy = pltpu.make_async_remote_copy(
                src_ref=src_of(peer),
                dst_ref=dst_of(d),
                send_sem=tp_ssem.at[phase, d - 1],
                recv_sem=tp_rsem.at[phase, d - 1],
                device_id=(ep, peer),
                device_id_type=MESH,
            )
            copy.start()
            copies.append(copy)
        return copies

    def over_ep(phase, src_of, dst_of):
        copies = []
        for d in range(1, n_ep):
            peer = lax.rem(ep + d, n_ep)
            copy = pltpu.make_async_remote_copy(
                src_ref=src_of(peer),
                dst_ref=dst_of(d),
                send_sem=ep_ssem.at[phase, d - 1],
                recv_sem=ep_rsem.at[phase, d - 1],
                device_id=(peer, tp),
                device_id_type=MESH,
            )
            copy.start()
            copies.append(copy)
        return copies

    def spread(axis, phase, buf):
        n, me = (n_tp, tp) if axis == "tp" else (n_ep, ep)
        ssem, rsem = (tp_ssem, tp_rsem) if axis == "tp" else (ep_ssem, ep_rsem)
        near = me + 1 - 2 * lax.rem(me, 2)
        half = n // 2

        def send(index, block, peer):
            copy = pltpu.make_async_remote_copy(
                src_ref=buf.at[block],
                dst_ref=buf.at[block],
                send_sem=ssem.at[phase, index],
                recv_sem=rsem.at[phase, index],
                device_id=(ep, peer) if axis == "tp" else (peer, tp),
                device_id_type=MESH,
            )
            copy.start()
            return copy

        copies = [send(m - 1, me, lax.rem(me + 2 * m, n)) for m in range(1, half)]
        copies.append(send(half - 1, me, near))
        for m in range(1, half):
            copies[m - 1].wait_recv()
            source = lax.rem(me - 2 * m + n, n)
            copies.append(send(half - 1 + m, source, near))
            yield source
        copies[half - 1].wait_recv()
        yield near
        for m in range(1, half):
            copies[half - 1 + m].wait_recv()
            yield lax.rem(near - 2 * m + n, n)
        sent.append(copies)

    sent = []

    def arrive(copies):
        for copy in copies:
            copy.wait_recv()

    for j in range(n_tp):
        p_send[j] = matmul(gated_ref[...], outw_ref[:, j * quarter : (j + 1) * quarter]).astype(bf16)
    pl.semaphore_wait(barrier, n_tp + n_ep - 2)
    c_part = over_tp(0, lambda peer: p_send.at[peer], lambda d: p_recv.at[d - 1])
    c_sel = over_ep(0, lambda peer: sel_ref.at[peer], lambda d: sel_recv.at[ep])
    sel_recv[ep] = sel_ref[ep]
    attended = p_send[tp].astype(f32)
    for d in range(1, n_tp):
        c_part[d - 1].wait_recv()
        attended = attended + p_recv[d - 1].astype(f32)
    middle = (hid_ref[:, own].astype(f32) + attended).astype(bf16).astype(f32)
    gain = gain_row[:, own]
    squares = jnp.sum(middle * middle, axis=-1, keepdims=True)
    inner = jnp.sum(middle * gain * gate_row[:, own], axis=-1, keepdims=True)
    lane = lax.broadcasted_iota(jnp.int32, (tokens, 128), 1)
    st_send[...] = jnp.where(lane < 64, squares, inner)
    c_stat = over_tp(1, lambda peer: st_send, lambda d: st_recv.at[d - 1])
    mid_buf[...] = middle
    totals = st_send[...]
    for d in range(1, n_tp):
        c_stat[d - 1].wait_recv()
        totals = totals + st_recv[d - 1]
    factor = lax.rsqrt(totals[:, 0:1] / width + EPSILON)
    br_buf[...] = jnp.broadcast_to(jax.nn.sigmoid(totals[:, 64:65] * factor), (tokens, 128))
    piece[ep] = (middle * factor * gain).astype(bf16)

    arrive(c_sel)

    def pick(source):
        picked = matmul(sel_recv[source][:, :tokens], piece[source]).astype(bf16)
        rows_all[tp, pl.ds(pl.multiple_of(source * cap, cap), cap), :] = picked

    pieces = spread("ep", 1, piece)
    first = next(pieces)
    pick(ep)
    pick(first)
    for source in pieces:
        pick(source)
    rows = spread("tp", 2, rows_all)
    loads[0].wait()
    loads[1].wait()
    everyone = piece[...].reshape(n_ep * tokens, quarter)
    units = dgw.shape[1]
    share = n_ep * tokens // n_tp
    next(rows)
    g_send[...] = matmul(everyone, dgw[...]).astype(bf16).reshape(n_tp, share, units)
    c_g = over_tp(3, lambda peer: g_send.at[peer], lambda d: g_recv.at[d - 1])
    u_send[...] = matmul(everyone, duw[...]).astype(bf16).reshape(n_tp, share, units)
    c_u = over_tp(4, lambda peer: u_send.at[peer], lambda d: u_recv.at[d - 1])

    loads[2].wait()
    loads[3].wait()
    for _ in rows:
        pass
    block = eg.shape[1]
    tile = 256 if block % 256 == 0 else 128

    @pl.loop(0, block // tile)
    def _(i):
        cols = pl.ds(pl.multiple_of(i * tile, tile), tile)
        gate_part = matmul(rows_all[0], eg[0:quarter, cols])
        up_part = matmul(rows_all[0], eu[0:quarter, cols])
        for j in range(1, n_tp):
            span = slice(j * quarter, (j + 1) * quarter)
            gate_part = gate_part + matmul(rows_all[j], eg[span, cols])
            up_part = up_part + matmul(rows_all[j], eu[span, cols])
        e_hid[:, cols] = (silu(gate_part) * up_part).astype(bf16)

    g_sum = g_send[tp].astype(f32)
    u_sum = u_send[tp].astype(f32)
    for d in range(1, n_tp):
        c_g[d - 1].wait_recv()
        g_sum = g_sum + g_recv[d - 1].astype(f32)
    for d in range(1, n_tp):
        c_u[d - 1].wait_recv()
        u_sum = u_sum + u_recv[d - 1].astype(f32)
    d_hid[tp] = (silu(g_sum) * u_sum).astype(bf16)
    held = spread("tp", 5, d_hid)
    next(held)

    loads[4].wait()
    for j in range(n_tp):
        eo_send[j] = matmul(e_hid[...], ed[:, j * quarter : (j + 1) * quarter]).astype(bf16)
    c_eo = over_tp(6, lambda peer: eo_send.at[peer], lambda d: eo_recv.at[d - 1])

    loads[5].wait()
    for _ in held:
        pass
    hidden = d_hid[...].reshape(n_ep * tokens, units)
    out_send[...] = matmul(hidden, ddw[...]).astype(bf16).reshape(n_ep, tokens, quarter)
    c_out = over_ep(2, lambda peer: out_send.at[peer], lambda d: out_recv.at[d - 1])

    summed = eo_send[tp].astype(f32)
    for d in range(1, n_tp):
        c_eo[d - 1].wait_recv()
        summed = summed + eo_recv[d - 1].astype(f32)
    ret_send[...] = summed.astype(bf16).reshape(n_ep, cap, quarter)
    c_ret = over_ep(3, lambda peer: ret_send.at[peer], lambda d: ret.at[ep])
    ret[ep] = ret_send[ep]

    dense = out_send[ep].astype(f32)
    for d in range(1, n_ep):
        c_out[d - 1].wait_recv()
        dense = dense + out_recv[d - 1].astype(f32)
    arrive(c_ret)
    answers = ret[...].reshape(n_ep * cap, quarter)
    over_items = (((0,), (0,)), ((), ()))
    routed = lax.dot_general(
        comb_hi_ref[...], answers, over_items, preferred_element_type=f32
    ) + lax.dot_general(comb_lo_ref[...], answers, over_items, preferred_element_type=f32)
    mixed_ref[...] = (mid_buf[...] + br_buf[:, 0:1] * dense + routed).astype(bf16)

    for copies in (c_part, c_sel, c_stat, c_g, c_u, c_eo, c_out, c_ret, *sent):
        for copy in copies:
            copy.wait_send()


def run_layer(gated, output_weight, hid, gain, gate, sel, comb_hi, comb_lo, eg, eu, ed, dg, du, dd):
    n_ep, n_tp = lax.axis_size("ep"), lax.axis_size("tp")
    tokens = hid.shape[0]
    quarter = hid.shape[1] // n_tp
    cap = sel.shape[1]
    items = n_ep * cap
    share = n_ep * tokens // n_tp
    units = dg.shape[1]
    bf16, f32 = jnp.bfloat16, jnp.float32
    vmem = pl.BlockSpec(memory_space=pltpu.VMEM)
    anyspace = pl.BlockSpec(memory_space=pl.ANY)
    scratch = [pltpu.VMEM(w.shape, bf16) for w in (eg, eu, ed, dg, du, dd)]
    scratch += [
        pltpu.VMEM(sel.shape, bf16),
        pltpu.VMEM((n_tp, tokens, quarter), bf16),
        pltpu.VMEM((n_tp - 1, tokens, quarter), bf16),
        pltpu.VMEM((tokens, 128), f32),
        pltpu.VMEM((n_tp - 1, tokens, 128), f32),
        pltpu.VMEM((tokens, quarter), f32),
        pltpu.VMEM((tokens, 128), f32),
        pltpu.VMEM((n_ep, tokens, quarter), bf16),
        pltpu.VMEM((n_tp, items, quarter), bf16),
        pltpu.VMEM((n_tp, share, units), bf16),
        pltpu.VMEM((n_tp - 1, share, units), bf16),
        pltpu.VMEM((n_tp, share, units), bf16),
        pltpu.VMEM((n_tp - 1, share, units), bf16),
        pltpu.VMEM((items, eg.shape[1]), bf16),
        pltpu.VMEM((n_tp, items, quarter), bf16),
        pltpu.VMEM((n_tp - 1, items, quarter), bf16),
        pltpu.VMEM((n_tp, share, units), bf16),
        pltpu.VMEM((n_ep, tokens, quarter), bf16),
        pltpu.VMEM((n_ep - 1, tokens, quarter), bf16),
        pltpu.VMEM((n_ep, cap, quarter), bf16),
        pltpu.VMEM((n_ep, cap, quarter), bf16),
        pltpu.SemaphoreType.DMA((6,)),
        pltpu.SemaphoreType.DMA((7, n_tp - 1)),
        pltpu.SemaphoreType.DMA((7, n_tp - 1)),
        pltpu.SemaphoreType.DMA((4, n_ep - 1)),
        pltpu.SemaphoreType.DMA((4, n_ep - 1)),
        pltpu.VMEM((1, hid.shape[1]), f32),
        pltpu.VMEM((1, hid.shape[1]), f32),
    ]
    return pl.pallas_call(
        functools.partial(layer_kernel, n_ep, n_tp),
        out_shape=jax.ShapeDtypeStruct((tokens, quarter), bf16),
        in_specs=[vmem] * 8 + [anyspace] * 6,
        out_specs=vmem,
        scratch_shapes=scratch,
        compiler_params=pltpu.CompilerParams(
            collective_id=0, has_side_effects=True, vmem_limit_bytes=60 * 1024 * 1024
        ),
    )(gated, output_weight, hid, gain, gate, sel, comb_hi, comb_lo, eg, eu, ed, dg, du, dd)


def attention_kernel(
    cap,
    hidden_ref,
    gain_ref,
    shift_ref,
    head_gain_ref,
    routes_ref,
    weights_ref,
    qw_hbm,
    kw_hbm,
    vw_hbm,
    ow_hbm,
    fw_hbm,
    state_hbm,
    gated_ref,
    sel_ref,
    comb_hi_ref,
    comb_lo_ref,
    new_hbm,
    qw,
    kw,
    vw,
    ow,
    fw,
    state,
    query,
    key,
    value,
    decay,
    readout,
    w_sem,
    in_sem,
    out_sem,
):
    f32, bf16 = jnp.float32, jnp.bfloat16
    tokens = hidden_ref.shape[0]
    heads, key_dim, value_dim = state.shape[1:]
    groups = tokens // 8
    loads = []
    pairs = ((fw_hbm, fw), (kw_hbm, kw), (qw_hbm, qw), (vw_hbm, vw), (ow_hbm, ow))
    for i, (src, dst) in enumerate(pairs):
        load = pltpu.make_async_copy(src, dst, w_sem.at[i])
        load.start()
        loads.append(load)

    def fetch(g):
        rows = pl.ds(g * 8, 8)
        return pltpu.make_async_copy(state_hbm.at[rows], state.at[rows], in_sem.at[g])

    def put(g):
        rows = pl.ds(g * 8, 8)
        return pltpu.make_async_copy(state.at[rows], new_hbm.at[rows], out_sem.at[g])

    for g in range(groups):
        fetch(g).start()

    inputs = hidden_ref[...].astype(f32)
    normed = (inputs * rms_factor(inputs) * flat_row(gain_ref)).astype(bf16)

    items = comb_hi_ref.shape[0]
    experts = (items // cap + 7) // 8 * 8
    first, second = routes_ref[0:1, :], routes_ref[1:2, :]
    expert = lax.broadcasted_iota(jnp.int32, (experts, tokens), 0)
    chosen0 = jnp.where(expert == first, 1.0, 0.0)
    chosen1 = jnp.where(expert == second, 1.0, 0.0)
    row = lax.broadcasted_iota(jnp.int32, (tokens, tokens), 0)
    col = lax.broadcasted_iota(jnp.int32, (tokens, tokens), 1)
    before = jnp.where(row < col, 1.0, 0.0).astype(bf16)
    earlier = matmul((chosen0 + chosen1).astype(bf16), before)
    slot0 = jnp.sum(earlier * chosen0, axis=0, keepdims=True)
    slot1 = jnp.sum(earlier * chosen1, axis=0, keepdims=True)
    table = lax.broadcasted_iota(jnp.int32, (items, tokens), 0)
    hit0 = table == first * cap + slot0.astype(jnp.int32)
    hit1 = table == second * cap + slot1.astype(jnp.int32)
    comb = jnp.where(hit0, weights_ref[0:1, :], 0.0) + jnp.where(hit1, weights_ref[1:2, :], 0.0)
    comb_hi = comb.astype(bf16)
    comb_hi_ref[...] = comb_hi
    comb_lo_ref[...] = (comb - comb_hi.astype(f32)).astype(bf16)
    sel_ref[...] = jnp.zeros(sel_ref.shape, bf16)
    sel_ref[:, :tokens] = (jnp.where(hit0, 1.0, 0.0) + jnp.where(hit1, 1.0, 0.0)).astype(bf16)

    def rounded_rows(weight):
        return matmul(normed, weight[...]).astype(bf16).astype(f32)

    loads[0].wait()
    drive = matmul(normed, fw[...])
    log_sig = jnp.minimum(drive, 0.0) - jnp.log1p(jnp.exp(-jnp.abs(drive)))
    decay[...] = jnp.exp(log_sig / TAU_DECAY + shift_ref[...]).reshape(decay.shape)
    loads[1].wait()
    key[...] = rounded_rows(kw).reshape(key.shape)
    loads[2].wait()
    query[...] = (rounded_rows(qw) * key_dim ** (-0.5)).reshape(query.shape)
    loads[3].wait()
    value[...] = rounded_rows(vw).reshape(value.shape)

    @pl.loop(0, groups)
    def _(g):
        fetch(g).wait()
        for h in range(heads):
            keys = slice(h * key_dim, (h + 1) * key_dim)
            vals = slice(h * value_dim, (h + 1) * value_dim)
            decay_cols = jnp.transpose(decay[g, :, keys])
            key_cols = jnp.transpose(key[g, :, keys])
            query_cols = jnp.transpose(query[g, :, keys])
            for j in range(8):
                fresh = (
                    decay_cols[:, j : j + 1] * state[g * 8 + j, h]
                    + key_cols[:, j : j + 1] * value[g, j : j + 1, vals]
                )
                state[g * 8 + j, h] = fresh
                readout[g, j : j + 1, vals] = jnp.sum(
                    query_cols[:, j : j + 1] * fresh, axis=0, keepdims=True
                )
        put(g).start()

    loads[4].wait()
    outgate = rounded_rows(ow)
    out = readout[...].reshape(tokens, heads * value_dim)
    for h in range(heads):
        vals = slice(h * value_dim, (h + 1) * value_dim)
        part = out[:, vals]
        gain = head_gain_ref[:, vals].astype(f32)
        gated_ref[:, vals] = (part * rms_factor(part) * gain * silu(outgate[:, vals])).astype(bf16)
    for g in range(groups):
        put(g).wait()


def run_attention(hidden, gain, shift, head_gain, routes, weights, qw, kw, vw, ow, fw, state, n_ep):
    bf16, f32 = jnp.bfloat16, jnp.float32
    tokens, heads, key_dim, value_dim = state.shape
    capacity = tokens * routes.shape[0] // n_ep + 2
    cap = (capacity + 15) // 16 * 16
    items = n_ep * cap
    groups = tokens // 8
    lanes = (tokens + 127) // 128 * 128
    vmem = pl.BlockSpec(memory_space=pltpu.VMEM)
    anyspace = pl.BlockSpec(memory_space=pl.ANY)
    gated, sel, comb_hi, comb_lo, new_state = pl.pallas_call(
        functools.partial(attention_kernel, cap),
        out_shape=(
            jax.ShapeDtypeStruct((tokens, heads * value_dim), bf16),
            jax.ShapeDtypeStruct((items, lanes), bf16),
            jax.ShapeDtypeStruct((items, tokens), bf16),
            jax.ShapeDtypeStruct((items, tokens), bf16),
            jax.ShapeDtypeStruct(state.shape, f32),
        ),
        in_specs=[vmem] * 6 + [anyspace] * 6,
        out_specs=(vmem, vmem, vmem, vmem, anyspace),
        scratch_shapes=[pltpu.VMEM(w.shape, bf16) for w in (qw, kw, vw, ow, fw)]
        + [
            pltpu.VMEM(state.shape, f32),
            pltpu.VMEM((groups, 8, heads * key_dim), f32),
            pltpu.VMEM((groups, 8, heads * key_dim), f32),
            pltpu.VMEM((groups, 8, heads * value_dim), f32),
            pltpu.VMEM((groups, 8, heads * key_dim), f32),
            pltpu.VMEM((groups, 8, heads * value_dim), f32),
            pltpu.SemaphoreType.DMA((5,)),
            pltpu.SemaphoreType.DMA((groups,)),
            pltpu.SemaphoreType.DMA((groups,)),
        ],
        compiler_params=pltpu.CompilerParams(vmem_limit_bytes=60 * 1024 * 1024),
    )(hidden, gain, shift, head_gain, routes, weights, qw, kw, vw, ow, fw, state)
    return gated, sel.reshape(n_ep, cap, lanes), comb_hi, comb_lo, new_state


def body(
    hidden_in,
    carried_state,
    input_gain,
    query_weight,
    key_weight,
    value_weight,
    outgate_weight,
    decay_weight,
    decay_shift,
    head_gain,
    output_weight,
    channel_gain,
    branch_gate,
    routes,
    route_weights,
    expert_gate,
    expert_up,
    expert_down,
    dense_gate,
    dense_up,
    dense_down,
):
    gated, sel, comb_hi, comb_lo, new_state = run_attention(
        hidden_in,
        input_gain.reshape(-1, 128),
        decay_shift,
        head_gain.reshape(1, -1),
        routes.T,
        route_weights.T,
        query_weight,
        key_weight,
        value_weight,
        outgate_weight,
        decay_weight,
        carried_state,
        lax.axis_size("ep"),
    )
    mixed = run_layer(
        gated,
        output_weight,
        hidden_in,
        channel_gain.reshape(-1, 128),
        branch_gate.reshape(-1, 128),
        sel,
        comb_hi,
        comb_lo,
        expert_gate[0],
        expert_up[0],
        expert_down[0],
        dense_gate,
        dense_up,
        dense_down,
    )
    return (mixed, new_state)


def solution(mesh):
    in_specs = (
        P("ep", None),
        P("ep", "tp", None, None),
        P(),
        P(None, "tp"),
        P(None, "tp"),
        P(None, "tp"),
        P(None, "tp"),
        P(None, "tp"),
        P("ep", "tp"),
        P("tp", None),
        P("tp", None),
        P(),
        P(),
        P("ep", None),
        P("ep", None),
        P("ep", None, "tp"),
        P("ep", None, "tp"),
        P("ep", "tp", None),
        P("tp", "ep"),
        P("tp", "ep"),
        P("ep", "tp"),
    )
    out_specs = (P("ep", "tp"), P("ep", "tp", None, None))
    return jax.shard_map(body, mesh=mesh, in_specs=in_specs, out_specs=out_specs, check_vma=False)
```

```python
import functools

import jax
import jax.numpy as jnp
from jax import lax
from jax.experimental import pallas as pl
from jax.experimental.pallas import tpu as pltpu
from jax.sharding import PartitionSpec as P

EPSILON = 1e-06
TAU_DECAY = 16.0
MESH = pl.DeviceIdType.MESH


def rms_factor(values):
    return lax.rsqrt(jnp.mean(values * values, axis=-1, keepdims=True) + EPSILON)


def matmul(left, right):
    return jnp.dot(left, right, preferred_element_type=jnp.float32)


def flat_row(ref):
    rows = ref[...].astype(jnp.float32)
    return jnp.concatenate([rows[k : k + 1, :] for k in range(rows.shape[0])], axis=1)


def silu(values):
    return values * jax.nn.sigmoid(values)


def layer_kernel(
    n_ep,
    n_tp,
    gated_ref,
    outw_ref,
    hid_ref,
    gain_ref,
    gate_ref,
    sel_ref,
    eg_hbm,
    eu_hbm,
    ed_hbm,
    dg_hbm,
    du_hbm,
    dd_hbm,
    mixed_ref,
    eg,
    eu,
    ed,
    wg,
    wu,
    ddw,
    gain_row,
    gate_row,
    sel_recv,
    p_send,
    p_recv,
    stat,
    scale_rows,
    mid_buf,
    piece,
    other,
    rows_all,
    row_scale,
    gu_send,
    gu_recv,
    gu_own,
    e_hid,
    near_send,
    near_recv,
    far_send,
    far_recv,
    eo_own,
    d_hid,
    d_out,
    y_send,
    y_recv,
    z_send,
    z_recv,
    w_sem,
    ssem,
    rsem,
):
    f32, bf16 = jnp.float32, jnp.bfloat16
    ep = lax.axis_index("ep")
    tp = lax.axis_index("tp")
    tokens, width = hid_ref.shape
    quarter = width // n_tp
    cap, lanes = sel_ref.shape[1:]
    units = dg_hbm.shape[1]
    n_z, half = n_ep // 2, n_tp // 2
    h, c = lax.div(tp, 2), lax.rem(tp, 2)
    partner = tp + 1 - 2 * c
    near = ep + 1 - 2 * lax.rem(ep, 2)
    steps = [0] + sorted(range(1, n_z), key=lambda m: abs(m - n_z // 2))
    own = pl.ds(pl.multiple_of(tp * quarter, quarter), quarter)

    def columns(q):
        return pl.ds(pl.multiple_of(q * quarter, quarter), quarter)

    def member(t, r):
        return lax.rem((near if r else ep) - 2 * steps[t] + n_ep, n_ep)

    def peer(dh, dc):
        return lax.rem(h + dh, half) * 2 + lax.rem(c + dc, 2)

    loads = []
    pairs = ((dg_hbm, wg.at[c]), (du_hbm, wu.at[c]), (eg_hbm, eg), (eu_hbm, eu))
    for i, (src, dst) in enumerate(pairs + ((ed_hbm, ed), (dd_hbm, ddw))):
        load = pltpu.make_async_copy(src, dst, w_sem.at[i])
        load.start()
        loads.append(load)

    gain_row[...] = flat_row(gain_ref)
    gate_row[...] = flat_row(gate_ref)
    barrier = pltpu.get_barrier_semaphore()
    for d in range(1, n_tp):
        pl.semaphore_signal(
            barrier, inc=1, device_id=(ep, lax.rem(tp + d, n_tp)), device_id_type=MESH
        )
    for d in range(1, n_ep):
        pl.semaphore_signal(
            barrier, inc=1, device_id=(lax.rem(ep + d, n_ep), tp), device_id_type=MESH
        )

    sent = []

    def send(src, dst, device):
        copy = pltpu.make_async_remote_copy(
            src_ref=src,
            dst_ref=dst,
            send_sem=ssem.at[len(sent)],
            recv_sem=rsem.at[len(sent)],
            device_id=device,
            device_id_type=MESH,
        )
        copy.start()
        sent.append(copy)
        return copy

    peers = [(dh, dc) for dh in range(1, half) for dc in range(2)] + [(0, 1)]
    for i, (dh, dc) in enumerate(peers):
        part = matmul(gated_ref[...], outw_ref[:, columns(peer(dh, dc))])
        p_send[i] = part.astype(bf16)
    pl.semaphore_wait(barrier, n_tp + n_ep - 2)
    c_part = []
    for i, (dh, dc) in enumerate(peers):
        c_part.append(send(p_send.at[i], p_recv.at[i], (ep, peer(dh, dc))))
    c_sel = []
    for d in range(1, n_ep):
        target = lax.rem(ep + d, n_ep)
        c_sel.append(send(sel_ref.at[target], sel_recv.at[ep], (target, tp)))
    c_dense = [
        send(dg_hbm, wg.at[c], (ep, partner)),
        send(du_hbm, wu.at[c], (ep, partner)),
    ]
    sel_recv[ep] = sel_ref[ep]
    attended = matmul(gated_ref[...], outw_ref[:, own]).astype(bf16).astype(f32)
    for i in reversed(range(len(peers))):
        c_part[i].wait_recv()
        attended = attended + p_recv[i].astype(f32)
    middle = (hid_ref[:, own].astype(f32) + attended).astype(bf16).astype(f32)
    shaped = middle * gain_row[:, own]
    piece[ep] = shaped.astype(bf16)
    squares = jnp.sum(middle * middle, axis=-1, keepdims=True)
    inner = jnp.sum(shaped * gate_row[:, own], axis=-1, keepdims=True)
    line = lax.broadcasted_iota(jnp.int32, (tokens, lanes), 0)
    lane = lax.broadcasted_iota(jnp.int32, (tokens, lanes), 1)
    eye = jnp.where(line == lane, 1.0, 0.0)
    stat[tp, ep, 0:1, :] = jnp.sum(eye * squares, axis=0, keepdims=True)
    stat[tp, ep, 1:2, :] = jnp.sum(eye * inner, axis=0, keepdims=True)
    c_near = send(piece.at[ep], piece.at[ep], (near, tp))
    c_stat = []
    for d in range(1, n_ep):
        target = lax.rem(ep + d, n_ep)
        c_stat.append(send(stat.at[tp, ep], stat.at[tp, ep], (target, tp)))
    c_z = [None]
    for t in range(1, n_z):
        target = lax.rem(ep + 2 * steps[t], n_ep)
        c_z.append(send(piece.at[ep], piece.at[ep], (target, tp)))
    mid_buf[...] = middle

    c_other = {}

    def share(t, r):
        block = member(t, r)
        c_other[t, r] = send(piece.at[block], other.at[block], (ep, partner))

    def pick(q, t, r, source):
        block = member(t, r)
        picked = matmul(sel_recv[block][:, :tokens], source[block]).astype(bf16)
        rows_all[q, (2 * t + r) * cap : (2 * t + r + 1) * cap, :] = picked

    share(0, 0)
    for copy in c_sel:
        copy.wait_recv()
    pick(tp, 0, 0, piece)
    c_near.wait_recv()
    share(0, 1)
    pick(tp, 0, 1, piece)
    c_relay = [None]
    for t in range(1, n_z):
        c_z[t].wait_recv()
        block = member(t, 0)
        c_relay.append(send(piece.at[block], piece.at[block], (near, tp)))
        share(t, 0)
        pick(tp, t, 0, piece)
    for copy in c_stat:
        copy.wait_recv()
    c_total = []
    for dh, dc in peers:
        c_total.append(send(stat.at[tp], stat.at[tp], (ep, peer(dh, dc))))

    groups = n_z // half
    per_part = n_z // 2
    c_rows, c_gu = {}, {}

    def send_rows(part):
        span = pl.ds(2 * part * per_part * cap, 2 * per_part * cap)
        for dh in range(1, half):
            q = peer(dh, 0)
            c_rows[part, dh] = send(rows_all.at[tp, span], rows_all.at[tp, span], (ep, q))

    def partial(j, dh):
        t = j * half + lax.rem(h + dh, half)
        m = steps[j * half]
        for k in range(1, half):
            m = jnp.where(t == j * half + k, steps[j * half + k], m)
        block = lax.rem(jnp.where(c == 1, near, ep) - 2 * m + n_ep, n_ep)
        left, right = piece[block], other[block]
        gate_part = matmul(left, wg[c]) + matmul(right, wg[1 - c])
        up_part = matmul(left, wu[c]) + matmul(right, wu[1 - c])
        return gate_part, up_part, block

    def send_partial(j):
        for dh in range(1, half):
            gate_part, up_part, _ = partial(j, dh)
            gu_send[j, dh - 1, 0] = gate_part.astype(bf16)
            gu_send[j, dh - 1, 1] = up_part.astype(bf16)
            source, target = gu_send.at[j, dh - 1], gu_recv.at[j, dh - 1]
            c_gu[j, dh] = send(source, target, (ep, peer(dh, 0)))

    def wait_other(ts):
        for t in ts:
            for r in range(2):
                c_other[t, r].wait_recv()

    ready = [False]

    def dense_ready():
        if not ready[0]:
            loads[0].wait()
            loads[1].wait()
            for copy in c_dense:
                copy.wait_recv()
            ready[0] = True

    for part in range(2):
        ts = range(part * per_part, (part + 1) * per_part)
        for t in ts:
            if t:
                c_relay[t].wait_recv()
                share(t, 1)
                pick(tp, t, 1, piece)
        send_rows(part)
        dense_ready()
        wait_other(ts)
        for j in range(part * groups // 2, (part + 1) * groups // 2):
            send_partial(j)
    blocks = []
    for j in range(groups):
        gate_part, up_part, block = partial(j, 0)
        gu_own[j, 0] = gate_part
        gu_own[j, 1] = up_part
        blocks.append(block)
    for t in range(n_z):
        for r in range(2):
            pick(partner, t, r, other)
    for copy in c_total:
        copy.wait_recv()
    totals = stat[0]
    for q in range(1, n_tp):
        totals = totals + stat[q]
    factors = lax.rsqrt(totals[:, 0:1, :] / width + EPSILON)
    scale_rows[:, 0:1, :] = factors
    scale_rows[:, 1:2, :] = jax.nn.sigmoid(totals[:, 1:2, :] * factors)
    for t in range(n_z):
        for r in range(2):
            block = member(t, r)
            chosen = sel_recv[block].astype(f32)
            chosen_lane = lax.broadcasted_iota(jnp.int32, (cap, lanes), 1)
            masked = jnp.where(chosen_lane < tokens, chosen * scale_rows[block, 0:1, :], 0.0)
            column = jnp.sum(masked, axis=1, keepdims=True)
            at = slice((2 * t + r) * cap, (2 * t + r + 1) * cap)
            row_scale[at, :] = jnp.broadcast_to(column, (cap, lanes))

    c_pass = []
    for part in range(2):
        span = pl.ds(2 * part * per_part * cap, 2 * per_part * cap)
        for dh in range(1, half):
            c_rows[part, dh].wait_recv()
            q = lax.rem(h - dh + half, half) * 2 + c
            c_pass.append(send(rows_all.at[q, span], rows_all.at[q, span], (ep, partner)))

    def column_of(row):
        return jnp.sum(eye * row, axis=1, keepdims=True)

    for j in range(groups):
        gate_sum, up_sum = gu_own[j, 0], gu_own[j, 1]
        for dh in range(1, half):
            c_gu[j, dh].wait_recv()
            gate_sum = gate_sum + gu_recv[j, dh - 1, 0].astype(f32)
            up_sum = up_sum + gu_recv[j, dh - 1, 1].astype(f32)
        scale = column_of(scale_rows[blocks[j], 0:1, :])
        d_hid[tp, j] = (silu(gate_sum * scale) * (up_sum * scale)).astype(bf16)
    c_hid = [send(d_hid.at[tp], d_hid.at[tp], (ep, peer(dh, 0))) for dh in range(1, half)]
    c_hid_near = [send(d_hid.at[tp], d_hid.at[tp], (ep, partner))]

    loads[2].wait()
    loads[3].wait()
    for copy in c_pass:
        copy.wait_recv()
    block = eg.shape[1]
    tile = 256 if block % 256 == 0 else 128

    @pl.loop(0, block // tile)
    def _(i):
        cols = pl.ds(pl.multiple_of(i * tile, tile), tile)
        gate_part = matmul(rows_all[0], eg[0:quarter, cols])
        up_part = matmul(rows_all[0], eu[0:quarter, cols])
        for q in range(1, n_tp):
            span = slice(q * quarter, (q + 1) * quarter)
            gate_part = gate_part + matmul(rows_all[q], eg[span, cols])
            up_part = up_part + matmul(rows_all[q], eu[span, cols])
        scale = row_scale[:, 0:1]
        e_hid[:, cols] = (silu(gate_part * scale) * (up_part * scale)).astype(bf16)

    loads[4].wait()
    c_near_eo = []
    for i, dh in enumerate(list(range(1, half)) + [0]):
        near_send[i] = matmul(e_hid[...], ed[:, columns(peer(dh, 1))]).astype(bf16)
        c_near_eo.append(send(near_send.at[i], near_recv.at[i], (ep, partner)))
    for dh in range(1, half):
        c_hid[dh - 1].wait_recv()
        q = lax.rem(h - dh + half, half) * 2 + c
        c_hid_near.append(send(d_hid.at[q], d_hid.at[q], (ep, partner)))
    c_far = []
    for i, dh in enumerate(range(1, half)):
        part = matmul(e_hid[...], ed[:, columns(peer(dh, 0))])
        c_near_eo[i].wait_recv()
        far_send[i] = (part + near_recv[i].astype(f32)).astype(bf16)
        c_far.append(send(far_send.at[i], far_recv.at[i], (ep, peer(dh, 0))))
    part = matmul(e_hid[...], ed[:, own])
    c_near_eo[half - 1].wait_recv()
    eo_own[...] = part + near_recv[half - 1].astype(f32)
    loads[5].wait()
    for copy in c_hid_near:
        copy.wait_recv()
    hidden = d_hid[...].reshape(n_ep * tokens, units)
    d_out[...] = matmul(hidden, ddw[...]).reshape(d_out.shape)
    total = eo_own[...]
    for i in range(half - 1):
        c_far[i].wait_recv()
        total = total + far_recv[i].astype(f32)
    eo_own[...] = total

    def outcome(t, r):
        block = member(t, r)
        span = slice((2 * t + r) * cap, (2 * t + r + 1) * cap)
        chosen = sel_recv[block]
        weight = chosen[:, lanes - 2 : lanes - 1].astype(f32)
        weight = weight + chosen[:, lanes - 1 : lanes].astype(f32)
        answers = (eo_own[span, :] * weight).astype(bf16)
        routed = lax.dot_general(
            chosen[:, :tokens], answers, (((0,), (0,)), ((), ())), preferred_element_type=f32
        )
        branch = column_of(scale_rows[block, 1:2, :])
        return branch * d_out[(t % half) * 2 + r, t // half] + routed

    order = list(range(1, n_z)) + [0]
    c_y = {}
    for t in order:
        y_send[t] = outcome(t, 1).astype(bf16)
        c_y[t] = send(y_send.at[t], y_recv.at[t], (near, tp))
    c_out = []
    for t in order:
        mine = outcome(t, 0)
        c_y[t].wait_recv()
        mine = mine + y_recv[t].astype(f32)
        if t:
            z_send[t - 1] = mine.astype(bf16)
            c_out.append(send(z_send.at[t - 1], z_recv.at[t - 1], (member(t, 0), tp)))
    mine = mine + mid_buf[...]
    for t in range(1, n_z):
        c_out[t - 1].wait_recv()
        mine = mine + z_recv[t - 1].astype(f32)
    mixed_ref[...] = mine.astype(bf16)
    for copy in sent:
        copy.wait_send()


def run_layer(gated, output_weight, hid, gain, gate, sel, eg, eu, ed, dg, du, dd):
    n_ep, n_tp = lax.axis_size("ep"), lax.axis_size("tp")
    tokens = hid.shape[0]
    quarter = hid.shape[1] // n_tp
    cap, lanes = sel.shape[1:]
    items = n_ep * cap
    n_z, half = n_ep // 2, n_tp // 2
    groups = n_z // half
    units = dg.shape[1]
    bf16, f32 = jnp.bfloat16, jnp.float32
    vmem = pl.BlockSpec(memory_space=pltpu.VMEM)
    anyspace = pl.BlockSpec(memory_space=pl.ANY)
    copies = 8 * n_ep + 4 * n_tp + 6 * n_z + 16
    scratch = [pltpu.VMEM(w.shape, bf16) for w in (eg, eu, ed)]
    scratch += [
        pltpu.VMEM((2, quarter, units), bf16),
        pltpu.VMEM((2, quarter, units), bf16),
        pltpu.VMEM(dd.shape, bf16),
        pltpu.VMEM((1, hid.shape[1]), f32),
        pltpu.VMEM((1, hid.shape[1]), f32),
        pltpu.VMEM(sel.shape, bf16),
        pltpu.VMEM((n_tp - 1, tokens, quarter), bf16),
        pltpu.VMEM((n_tp - 1, tokens, quarter), bf16),
        pltpu.VMEM((n_tp, n_ep, 2, lanes), f32),
        pltpu.VMEM((n_ep, 2, lanes), f32),
        pltpu.VMEM((tokens, quarter), f32),
        pltpu.VMEM((n_ep, tokens, quarter), bf16),
        pltpu.VMEM((n_ep, tokens, quarter), bf16),
        pltpu.VMEM((n_tp, items, quarter), bf16),
        pltpu.VMEM((items, lanes), f32),
        pltpu.VMEM((groups, half - 1, 2, tokens, units), bf16),
        pltpu.VMEM((groups, half - 1, 2, tokens, units), bf16),
        pltpu.VMEM((groups, 2, tokens, units), f32),
        pltpu.VMEM((items, eg.shape[1]), bf16),
        pltpu.VMEM((half, items, quarter), bf16),
        pltpu.VMEM((half, items, quarter), bf16),
        pltpu.VMEM((half - 1, items, quarter), bf16),
        pltpu.VMEM((half - 1, items, quarter), bf16),
        pltpu.VMEM((items, quarter), f32),
        pltpu.VMEM((n_tp, groups, tokens, units), bf16),
        pltpu.VMEM((n_tp, groups, tokens, quarter), f32),
        pltpu.VMEM((n_z, tokens, quarter), bf16),
        pltpu.VMEM((n_z, tokens, quarter), bf16),
        pltpu.VMEM((n_z - 1, tokens, quarter), bf16),
        pltpu.VMEM((n_z - 1, tokens, quarter), bf16),
        pltpu.SemaphoreType.DMA((6,)),
        pltpu.SemaphoreType.DMA((copies,)),
        pltpu.SemaphoreType.DMA((copies,)),
    ]
    return pl.pallas_call(
        functools.partial(layer_kernel, n_ep, n_tp),
        out_shape=jax.ShapeDtypeStruct((tokens, quarter), bf16),
        in_specs=[vmem] * 6 + [anyspace] * 6,
        out_specs=vmem,
        scratch_shapes=scratch,
        compiler_params=pltpu.CompilerParams(
            collective_id=0, has_side_effects=True, vmem_limit_bytes=60 * 1024 * 1024
        ),
    )(gated, output_weight, hid, gain, gate, sel, eg, eu, ed, dg, du, dd)


def attention_kernel(
    cap,
    hidden_ref,
    gain_ref,
    shift_ref,
    head_gain_ref,
    routes_ref,
    weights_ref,
    qw_hbm,
    kw_hbm,
    vw_hbm,
    ow_hbm,
    fw_hbm,
    state_hbm,
    gated_ref,
    sel_ref,
    new_hbm,
    qw,
    kw,
    vw,
    ow,
    fw,
    state,
    query,
    key,
    value,
    decay,
    readout,
    w_sem,
    in_sem,
    out_sem,
):
    f32, bf16 = jnp.float32, jnp.bfloat16
    tokens = hidden_ref.shape[0]
    heads, key_dim, value_dim = state.shape[1:]
    groups = tokens // 8
    loads = []
    pairs = ((fw_hbm, fw), (kw_hbm, kw), (qw_hbm, qw), (vw_hbm, vw), (ow_hbm, ow))
    for i, (src, dst) in enumerate(pairs):
        load = pltpu.make_async_copy(src, dst, w_sem.at[i])
        load.start()
        loads.append(load)

    def fetch(g):
        rows = pl.ds(g * 8, 8)
        return pltpu.make_async_copy(state_hbm.at[rows], state.at[rows], in_sem.at[g])

    def put(g):
        rows = pl.ds(g * 8, 8)
        return pltpu.make_async_copy(state.at[rows], new_hbm.at[rows], out_sem.at[g])

    for g in range(groups):
        fetch(g).start()

    inputs = hidden_ref[...].astype(f32)
    normed = (inputs * rms_factor(inputs) * flat_row(gain_ref)).astype(bf16)

    items, lanes = sel_ref.shape
    experts = (items // cap + 7) // 8 * 8
    first, second = routes_ref[0:1, :], routes_ref[1:2, :]
    expert = lax.broadcasted_iota(jnp.int32, (experts, tokens), 0)
    chosen0 = jnp.where(expert == first, 1.0, 0.0)
    chosen1 = jnp.where(expert == second, 1.0, 0.0)
    row = lax.broadcasted_iota(jnp.int32, (tokens, tokens), 0)
    col = lax.broadcasted_iota(jnp.int32, (tokens, tokens), 1)
    before = jnp.where(row < col, 1.0, 0.0).astype(bf16)
    earlier = matmul((chosen0 + chosen1).astype(bf16), before)
    slot0 = jnp.sum(earlier * chosen0, axis=0, keepdims=True)
    slot1 = jnp.sum(earlier * chosen1, axis=0, keepdims=True)
    table = lax.broadcasted_iota(jnp.int32, (items, tokens), 0)
    hit0 = table == first * cap + slot0.astype(jnp.int32)
    hit1 = table == second * cap + slot1.astype(jnp.int32)
    comb = jnp.where(hit0, weights_ref[0:1, :], 0.0) + jnp.where(hit1, weights_ref[1:2, :], 0.0)
    weight = jnp.sum(comb, axis=1, keepdims=True)
    weight_hi = weight.astype(bf16).astype(f32)
    lane = lax.broadcasted_iota(jnp.int32, (items, lanes), 1)
    tail = jnp.where(lane == lanes - 2, weight_hi, weight - weight_hi)
    sel_ref[...] = jnp.where(lane < lanes - 2, 0.0, tail).astype(bf16)
    sel_ref[:, :tokens] = (jnp.where(hit0, 1.0, 0.0) + jnp.where(hit1, 1.0, 0.0)).astype(bf16)

    def rounded_rows(weight):
        return matmul(normed, weight[...]).astype(bf16).astype(f32)

    loads[0].wait()
    drive = matmul(normed, fw[...])
    log_sig = jnp.minimum(drive, 0.0) - jnp.log1p(jnp.exp(-jnp.abs(drive)))
    decay[...] = jnp.exp(log_sig / TAU_DECAY + shift_ref[...]).reshape(decay.shape)
    loads[1].wait()
    key[...] = rounded_rows(kw).reshape(key.shape)
    loads[2].wait()
    query[...] = (rounded_rows(qw) * key_dim ** (-0.5)).reshape(query.shape)
    loads[3].wait()
    value[...] = rounded_rows(vw).reshape(value.shape)

    @pl.loop(0, groups)
    def _(g):
        fetch(g).wait()
        for h in range(heads):
            keys = slice(h * key_dim, (h + 1) * key_dim)
            vals = slice(h * value_dim, (h + 1) * value_dim)
            decay_cols = jnp.transpose(decay[g, :, keys])
            key_cols = jnp.transpose(key[g, :, keys])
            query_cols = jnp.transpose(query[g, :, keys])
            for j in range(8):
                fresh = (
                    decay_cols[:, j : j + 1] * state[g * 8 + j, h]
                    + key_cols[:, j : j + 1] * value[g, j : j + 1, vals]
                )
                state[g * 8 + j, h] = fresh
                readout[g, j : j + 1, vals] = jnp.sum(
                    query_cols[:, j : j + 1] * fresh, axis=0, keepdims=True
                )
        put(g).start()

    loads[4].wait()
    outgate = rounded_rows(ow)
    out = readout[...].reshape(tokens, heads * value_dim)
    for h in range(heads):
        vals = slice(h * value_dim, (h + 1) * value_dim)
        part = out[:, vals]
        gain = head_gain_ref[:, vals].astype(f32)
        gated_ref[:, vals] = (part * rms_factor(part) * gain * silu(outgate[:, vals])).astype(bf16)
    for g in range(groups):
        put(g).wait()


def run_attention(hidden, gain, shift, head_gain, routes, weights, qw, kw, vw, ow, fw, state, n_ep):
    bf16, f32 = jnp.bfloat16, jnp.float32
    tokens, heads, key_dim, value_dim = state.shape
    capacity = tokens * routes.shape[0] // n_ep + 2
    cap = (capacity + 15) // 16 * 16
    items = n_ep * cap
    groups = tokens // 8
    lanes = (tokens + 2 + 127) // 128 * 128
    vmem = pl.BlockSpec(memory_space=pltpu.VMEM)
    anyspace = pl.BlockSpec(memory_space=pl.ANY)
    gated, sel, new_state = pl.pallas_call(
        functools.partial(attention_kernel, cap),
        out_shape=(
            jax.ShapeDtypeStruct((tokens, heads * value_dim), bf16),
            jax.ShapeDtypeStruct((items, lanes), bf16),
            jax.ShapeDtypeStruct(state.shape, f32),
        ),
        in_specs=[vmem] * 6 + [anyspace] * 6,
        out_specs=(vmem, vmem, anyspace),
        scratch_shapes=[pltpu.VMEM(w.shape, bf16) for w in (qw, kw, vw, ow, fw)]
        + [
            pltpu.VMEM(state.shape, f32),
            pltpu.VMEM((groups, 8, heads * key_dim), f32),
            pltpu.VMEM((groups, 8, heads * key_dim), f32),
            pltpu.VMEM((groups, 8, heads * value_dim), f32),
            pltpu.VMEM((groups, 8, heads * key_dim), f32),
            pltpu.VMEM((groups, 8, heads * value_dim), f32),
            pltpu.SemaphoreType.DMA((5,)),
            pltpu.SemaphoreType.DMA((groups,)),
            pltpu.SemaphoreType.DMA((groups,)),
        ],
        compiler_params=pltpu.CompilerParams(vmem_limit_bytes=60 * 1024 * 1024),
    )(hidden, gain, shift, head_gain, routes, weights, qw, kw, vw, ow, fw, state)
    return gated, sel.reshape(n_ep, cap, lanes), new_state


def body(
    hidden_in,
    carried_state,
    input_gain,
    query_weight,
    key_weight,
    value_weight,
    outgate_weight,
    decay_weight,
    decay_shift,
    head_gain,
    output_weight,
    channel_gain,
    branch_gate,
    routes,
    route_weights,
    expert_gate,
    expert_up,
    expert_down,
    dense_gate,
    dense_up,
    dense_down,
):
    gated, sel, new_state = run_attention(
        hidden_in,
        input_gain.reshape(-1, 128),
        decay_shift,
        head_gain.reshape(1, -1),
        routes.T,
        route_weights.T,
        query_weight,
        key_weight,
        value_weight,
        outgate_weight,
        decay_weight,
        carried_state,
        lax.axis_size("ep"),
    )
    mixed = run_layer(
        gated,
        output_weight,
        hidden_in,
        channel_gain.reshape(-1, 128),
        branch_gate.reshape(-1, 128),
        sel,
        expert_gate[0],
        expert_up[0],
        expert_down[0],
        dense_gate,
        dense_up,
        dense_down,
    )
    return (mixed, new_state)


def solution(mesh):
    in_specs = (
        P("ep", None),
        P("ep", "tp", None, None),
        P(),
        P(None, "tp"),
        P(None, "tp"),
        P(None, "tp"),
        P(None, "tp"),
        P(None, "tp"),
        P("ep", "tp"),
        P("tp", None),
        P("tp", None),
        P(),
        P(),
        P("ep", None),
        P("ep", None),
        P("ep", None, "tp"),
        P("ep", None, "tp"),
        P("ep", "tp", None),
        P("tp", "ep"),
        P("tp", "ep"),
        P("ep", "tp"),
    )
    out_specs = (P("ep", "tp"), P("ep", "tp", None, None))
    return jax.shard_map(body, mesh=mesh, in_specs=in_specs, out_specs=out_specs, check_vma=False)
```

```python
import functools

import jax
import jax.numpy as jnp
from jax import lax
from jax.experimental import pallas as pl
from jax.experimental.pallas import tpu as pltpu
from jax.sharding import PartitionSpec as P

EPSILON = 1e-06
TAU_DECAY = 16.0
MESH = pl.DeviceIdType.MESH


def rms_factor(values):
    return lax.rsqrt(jnp.mean(values * values, axis=-1, keepdims=True) + EPSILON)


def matmul(left, right):
    return jnp.dot(left, right, preferred_element_type=jnp.float32)


def flat_row(ref):
    rows = ref[...].astype(jnp.float32)
    return jnp.concatenate([rows[k : k + 1, :] for k in range(rows.shape[0])], axis=1)


def silu(values):
    return values * jax.nn.sigmoid(values)


def layer_kernel(
    n_ep,
    n_tp,
    gated_ref,
    outw_ref,
    hid_ref,
    gain_ref,
    gate_ref,
    sel_ref,
    eg_hbm,
    eu_hbm,
    ed_hbm,
    dg_hbm,
    du_hbm,
    dd_hbm,
    mixed_ref,
    eg,
    eu,
    ed,
    wg,
    wu,
    ddw,
    gain_row,
    gate_row,
    sel_recv,
    p_send,
    p_recv,
    stat,
    scale_rows,
    mid_buf,
    piece,
    other,
    rows_all,
    row_scale,
    gu_send,
    gu_recv,
    gu_own,
    e_hid,
    near_send,
    near_recv,
    far_send,
    far_recv,
    eo_own,
    d_hid,
    d_out,
    y_send,
    y_recv,
    z_send,
    z_recv,
    w_sem,
    ssem,
    rsem,
):
    f32, bf16 = jnp.float32, jnp.bfloat16
    ep = lax.axis_index("ep")
    tp = lax.axis_index("tp")
    tokens, width = hid_ref.shape
    quarter = width // n_tp
    cap, lanes = sel_ref.shape[1:]
    units = dg_hbm.shape[1]
    n_z, half = n_ep // 2, n_tp // 2
    h, c = lax.div(tp, 2), lax.rem(tp, 2)
    partner = tp + 1 - 2 * c
    near = ep + 1 - 2 * lax.rem(ep, 2)
    steps = [0] + sorted(range(1, n_z), key=lambda m: abs(m - n_z // 2))
    own = pl.ds(pl.multiple_of(tp * quarter, quarter), quarter)

    def columns(q):
        return pl.ds(pl.multiple_of(q * quarter, quarter), quarter)

    def member(t, r):
        return lax.rem((near if r else ep) - 2 * steps[t] + n_ep, n_ep)

    def peer(dh, dc):
        return lax.rem(h + dh, half) * 2 + lax.rem(c + dc, 2)

    loads = []
    pairs = ((dg_hbm, wg.at[c]), (du_hbm, wu.at[c]), (eg_hbm, eg), (eu_hbm, eu))
    for i, (src, dst) in enumerate(pairs + ((ed_hbm, ed), (dd_hbm, ddw))):
        load = pltpu.make_async_copy(src, dst, w_sem.at[i])
        load.start()
        loads.append(load)

    gain_row[...] = flat_row(gain_ref)
    gate_row[...] = flat_row(gate_ref)
    barrier = pltpu.get_barrier_semaphore()
    for d in range(1, n_tp):
        pl.semaphore_signal(
            barrier, inc=1, device_id=(ep, lax.rem(tp + d, n_tp)), device_id_type=MESH
        )
    for d in range(1, n_ep):
        pl.semaphore_signal(
            barrier, inc=1, device_id=(lax.rem(ep + d, n_ep), tp), device_id_type=MESH
        )

    sent = []

    def send(src, dst, device):
        copy = pltpu.make_async_remote_copy(
            src_ref=src,
            dst_ref=dst,
            send_sem=ssem.at[len(sent)],
            recv_sem=rsem.at[len(sent)],
            device_id=device,
            device_id_type=MESH,
        )
        copy.start()
        sent.append(copy)
        return copy

    peers = [(dh, dc) for dh in range(1, half) for dc in range(2)] + [(0, 1)]
    for i, (dh, dc) in enumerate(peers):
        part = matmul(gated_ref[...], outw_ref[:, columns(peer(dh, dc))])
        p_send[i] = part.astype(bf16)
    pl.semaphore_wait(barrier, n_tp + n_ep - 2)
    c_part = []
    for i, (dh, dc) in enumerate(peers):
        c_part.append(send(p_send.at[i], p_recv.at[i], (ep, peer(dh, dc))))
    c_sel = []
    for d in range(1, n_ep):
        target = lax.rem(ep + d, n_ep)
        c_sel.append(send(sel_ref.at[target], sel_recv.at[ep], (target, tp)))
    c_dense = [
        send(dg_hbm, wg.at[c], (ep, partner)),
        send(du_hbm, wu.at[c], (ep, partner)),
    ]
    sel_recv[ep] = sel_ref[ep]
    attended = matmul(gated_ref[...], outw_ref[:, own]).astype(bf16).astype(f32)
    for i in reversed(range(len(peers))):
        c_part[i].wait_recv()
        attended = attended + p_recv[i].astype(f32)
    middle = (hid_ref[:, own].astype(f32) + attended).astype(bf16).astype(f32)
    shaped = middle * gain_row[:, own]
    piece[ep] = shaped.astype(bf16)
    squares = jnp.sum(middle * middle, axis=-1, keepdims=True)
    inner = jnp.sum(shaped * gate_row[:, own], axis=-1, keepdims=True)
    line = lax.broadcasted_iota(jnp.int32, (tokens, lanes), 0)
    lane = lax.broadcasted_iota(jnp.int32, (tokens, lanes), 1)
    eye = jnp.where(line == lane, 1.0, 0.0)
    stat[tp, ep, 0:1, :] = jnp.sum(eye * squares, axis=0, keepdims=True)
    stat[tp, ep, 1:2, :] = jnp.sum(eye * inner, axis=0, keepdims=True)
    c_near = send(piece.at[ep], piece.at[ep], (near, tp))
    c_stat = []
    for d in range(1, n_ep):
        target = lax.rem(ep + d, n_ep)
        c_stat.append(send(stat.at[tp, ep], stat.at[tp, ep], (target, tp)))
    c_z = [None]
    for t in range(1, n_z):
        target = lax.rem(ep + 2 * steps[t], n_ep)
        c_z.append(send(piece.at[ep], piece.at[ep], (target, tp)))
    mid_buf[...] = middle

    c_other = {}

    def share(t, r):
        block = member(t, r)
        c_other[t, r] = send(piece.at[block], other.at[block], (ep, partner))

    def pick(q, t, r, source):
        block = member(t, r)
        picked = matmul(sel_recv[block][:, :tokens], source[block]).astype(bf16)
        rows_all[q, (2 * t + r) * cap : (2 * t + r + 1) * cap, :] = picked

    c_rows, c_pass, c_gu, c_hid, c_hid_near = {}, {}, {}, {}, {}
    c_eo_near, c_eo_far, c_y, c_out = {}, {}, {}, {}
    sub = tokens // half
    per_part = n_z // 2
    parts = [range(p * per_part, (p + 1) * per_part) for p in range(2)]

    def of_chip(value, index):
        chosen = value[:sub]
        for k in range(1, half):
            chosen = jnp.where(index == k, value[k * sub : (k + 1) * sub], chosen)
        return chosen

    def span_of(t):
        return pl.ds(2 * t * cap, 2 * cap)

    def send_rows(t):
        for dh in range(1, half):
            rows = rows_all.at[tp, span_of(t)]
            c_rows[t, dh] = send(rows, rows, (ep, peer(dh, 0)))

    def pass_rows(t):
        for dh in range(1, half):
            c_rows[t, dh].wait_recv()
            q = lax.rem(h - dh + half, half) * 2 + c
            rows = rows_all.at[q, span_of(t)]
            c_pass[t, dh] = send(rows, rows, (ep, partner))

    def partial(t):
        for r in range(2):
            c_other[t, r].wait_recv()
        block = lax.rem(jnp.where(c == 1, near, ep) - 2 * steps[t] + n_ep, n_ep)
        left, right = piece[block], other[block]
        for i, w in enumerate((wg, wu)):
            product = matmul(left, w[c]) + matmul(right, w[1 - c])
            gu_own[t, i] = of_chip(product, h)
            for dh in range(1, half):
                gu_send[t, dh - 1, i] = of_chip(product, lax.rem(h + dh, half)).astype(bf16)
        for dh in range(1, half):
            source, target = gu_send.at[t, dh - 1], gu_recv.at[t, dh - 1]
            c_gu[t, dh] = send(source, target, (ep, peer(dh, 0)))

    line_own = lax.broadcasted_iota(jnp.int32, (sub, lanes), 0) + h * sub
    eye_own = jnp.where(line_own == lax.broadcasted_iota(jnp.int32, (sub, lanes), 1), 1.0, 0.0)

    def activate(p):
        shares = []
        for t in parts[p]:
            gate_sum, up_sum = gu_own[t, 0], gu_own[t, 1]
            for dh in range(1, half):
                c_gu[t, dh].wait_recv()
                gate_sum = gate_sum + gu_recv[t, dh - 1, 0].astype(f32)
                up_sum = up_sum + gu_recv[t, dh - 1, 1].astype(f32)
            block = lax.rem(jnp.where(c == 1, near, ep) - 2 * steps[t] + n_ep, n_ep)
            scale = jnp.sum(eye_own * scale_rows[block, 0:1, :], axis=1, keepdims=True)
            shares.append(silu(gate_sum * scale) * (up_sum * scale))
        d_hid[tp, p] = jnp.concatenate(shares, axis=0).astype(bf16)
        mine = d_hid.at[tp, p]
        for dh in range(1, half):
            c_hid[p, dh] = send(mine, mine, (ep, peer(dh, 0)))
        c_hid_near[p, 0] = send(mine, mine, (ep, partner))

    def pass_hidden(p):
        for dh in range(1, half):
            c_hid[p, dh].wait_recv()
            got = d_hid.at[lax.rem(h - dh + half, half) * 2 + c, p]
            c_hid_near[p, dh] = send(got, got, (ep, partner))

    def dense_down(p):
        for dh in range(half):
            c_hid_near[p, dh].wait_recv()
        hidden = d_hid[:, p].reshape(n_tp * per_part * sub, units)
        d_out[p] = matmul(hidden, ddw[...]).reshape(d_out.shape[1:])

    def scales():
        for copy in c_total:
            copy.wait_recv()
        totals = stat[0]
        for q in range(1, n_tp):
            totals = totals + stat[q]
        factors = lax.rsqrt(totals[:, 0:1, :] / width + EPSILON)
        scale_rows[:, 0:1, :] = factors
        scale_rows[:, 1:2, :] = jax.nn.sigmoid(totals[:, 1:2, :] * factors)

    count = 2 * per_part * cap
    chosen_lane = lax.broadcasted_iota(jnp.int32, (cap, lanes), 1)

    def prepare(p):
        for t in parts[p]:
            for r in range(2):
                pick(partner, t, r, other)
                block = member(t, r)
                chosen = sel_recv[block].astype(f32)
                masked = jnp.where(chosen_lane < tokens, chosen * scale_rows[block, 0:1, :], 0.0)
                column = jnp.sum(masked, axis=1, keepdims=True)
                at = slice((2 * t + r) * cap, (2 * t + r + 1) * cap)
                row_scale[at, :] = jnp.broadcast_to(column, (cap, lanes))

    inner_width = eg.shape[1]
    tile = 256 if inner_width % 256 == 0 else 128

    def expert_in(p):
        for t in parts[p]:
            for dh in range(1, half):
                c_pass[t, dh].wait_recv()
        at = slice(p * count, (p + 1) * count)

        scale = row_scale[at, 0:1]
        for i in range(inner_width // tile):
            cols = slice(i * tile, (i + 1) * tile)
            gate_part = matmul(rows_all[0, at], eg[0:quarter, cols])
            up_part = matmul(rows_all[0, at], eu[0:quarter, cols])
            for q in range(1, n_tp):
                span = slice(q * quarter, (q + 1) * quarter)
                gate_part = gate_part + matmul(rows_all[q, at], eg[span, cols])
                up_part = up_part + matmul(rows_all[q, at], eu[span, cols])
            e_hid[at, cols] = (silu(gate_part * scale) * (up_part * scale)).astype(bf16)

    def expert_near(p):
        at = slice(p * count, (p + 1) * count)
        for i, dh in enumerate(list(range(1, half)) + [0]):
            near_send[p, i] = matmul(e_hid[at, :], ed[:, columns(peer(dh, 1))]).astype(bf16)
            source, target = near_send.at[p, i], near_recv.at[p, i]
            c_eo_near[p, i] = send(source, target, (ep, partner))

    def expert_far(p):
        at = slice(p * count, (p + 1) * count)
        for i, dh in enumerate(range(1, half)):
            part = matmul(e_hid[at, :], ed[:, columns(peer(dh, 0))])
            c_eo_near[p, i].wait_recv()
            far_send[p, i] = (part + near_recv[p, i].astype(f32)).astype(bf16)
            source, target = far_send.at[p, i], far_recv.at[p, i]
            c_eo_far[p, i] = send(source, target, (ep, peer(dh, 0)))
        part = matmul(e_hid[at, :], ed[:, own])
        c_eo_near[p, half - 1].wait_recv()
        eo_own[at, :] = part + near_recv[p, half - 1].astype(f32)

    def expert_total(p):
        at = slice(p * count, (p + 1) * count)
        total = eo_own[at, :]
        for i in range(half - 1):
            c_eo_far[p, i].wait_recv()
            total = total + far_recv[p, i].astype(f32)
        eo_own[at, :] = total

    def outcome(t, r):
        block = member(t, r)
        span = slice((2 * t + r) * cap, (2 * t + r + 1) * cap)
        chosen = sel_recv[block]
        weight = chosen[:, lanes - 2 : lanes - 1].astype(f32)
        weight = weight + chosen[:, lanes - 1 : lanes].astype(f32)
        answers = (eo_own[span, :] * weight).astype(bf16)
        routed = lax.dot_general(
            chosen[:, :tokens], answers, (((0,), (0,)), ((), ())), preferred_element_type=f32
        )
        branch = jnp.sum(eye * scale_rows[block, 1:2, :], axis=1, keepdims=True)
        p, k = t // per_part, t % per_part
        dense = [d_out[p, 2 * j + r, k * sub : (k + 1) * sub, :] for j in range(half)]
        return branch * jnp.concatenate(dense, axis=0) + routed

    def far_first(p):
        return [t for t in parts[p] if t] + [t for t in parts[p] if not t]

    def send_near(p):
        for t in far_first(p):
            y_send[t] = outcome(t, 1).astype(bf16)
            c_y[t] = send(y_send.at[t], y_recv.at[t], (near, tp))

    def send_out(p):
        for t in far_first(p):
            mine = outcome(t, 0)
            c_y[t].wait_recv()
            mine = mine + y_recv[t].astype(f32)
            if t:
                z_send[t - 1] = mine.astype(bf16)
                c_out[t] = send(z_send.at[t - 1], z_recv.at[t - 1], (member(t, 0), tp))
            else:
                mid_buf[...] = mid_buf[...] + mine

    share(0, 0)
    for copy in c_sel:
        copy.wait_recv()
    pick(tp, 0, 0, piece)
    c_near.wait_recv()
    share(0, 1)
    pick(tp, 0, 1, piece)
    send_rows(0)
    c_relay = [None]
    for t in range(1, n_z):
        c_z[t].wait_recv()
        block = member(t, 0)
        c_relay.append(send(piece.at[block], piece.at[block], (near, tp)))
        share(t, 0)
        pick(tp, t, 0, piece)
        if t == 1:
            loads[0].wait()
            loads[1].wait()
            for copy in c_dense:
                copy.wait_recv()
            partial(0)
    for copy in c_stat:
        copy.wait_recv()
    c_total = []
    for dh, dc in peers:
        c_total.append(send(stat.at[tp], stat.at[tp], (ep, peer(dh, dc))))
    for t in range(1, n_z):
        c_relay[t].wait_recv()
        share(t, 1)
        pick(tp, t, 1, piece)
        send_rows(t)
        if t > 1:
            partial(t - 1)
        if t != 2:
            pass_rows(max(t - 2, 0))
    scales()
    prepare(0)
    for t in range(max(n_z - 2, 1), per_part):
        pass_rows(t)
    partial(n_z - 1)
    loads[2].wait()
    loads[3].wait()
    expert_in(0)
    for t in range(max(n_z - 2, per_part), n_z):
        pass_rows(t)
    loads[4].wait()
    expert_near(0)
    activate(0)
    prepare(1)
    expert_far(0)
    activate(1)
    expert_in(1)
    expert_near(1)
    pass_hidden(0)
    expert_far(1)
    loads[5].wait()
    dense_down(0)
    expert_total(0)
    send_near(0)
    pass_hidden(1)
    dense_down(1)
    expert_total(1)
    send_near(1)
    send_out(0)
    send_out(1)
    mine = mid_buf[...]
    for t in range(1, n_z):
        c_out[t].wait_recv()
        mine = mine + z_recv[t - 1].astype(f32)
    mixed_ref[...] = mine.astype(bf16)
    for copy in sent:
        copy.wait_send()


def run_layer(gated, output_weight, hid, gain, gate, sel, eg, eu, ed, dg, du, dd):
    n_ep, n_tp = lax.axis_size("ep"), lax.axis_size("tp")
    tokens = hid.shape[0]
    quarter = hid.shape[1] // n_tp
    cap, lanes = sel.shape[1:]
    items = n_ep * cap
    n_z, half = n_ep // 2, n_tp // 2
    sub = tokens // half
    part = items // 2
    units = dg.shape[1]
    bf16, f32 = jnp.bfloat16, jnp.float32
    vmem = pl.BlockSpec(memory_space=pltpu.VMEM)
    anyspace = pl.BlockSpec(memory_space=pl.ANY)
    copies = 8 * n_ep + 4 * n_tp + 6 * n_z + 16
    scratch = [pltpu.VMEM(w.shape, bf16) for w in (eg, eu, ed)]
    scratch += [
        pltpu.VMEM((2, quarter, units), bf16),
        pltpu.VMEM((2, quarter, units), bf16),
        pltpu.VMEM(dd.shape, bf16),
        pltpu.VMEM((1, hid.shape[1]), f32),
        pltpu.VMEM((1, hid.shape[1]), f32),
        pltpu.VMEM(sel.shape, bf16),
        pltpu.VMEM((n_tp - 1, tokens, quarter), bf16),
        pltpu.VMEM((n_tp - 1, tokens, quarter), bf16),
        pltpu.VMEM((n_tp, n_ep, 2, lanes), f32),
        pltpu.VMEM((n_ep, 2, lanes), f32),
        pltpu.VMEM((tokens, quarter), f32),
        pltpu.VMEM((n_ep, tokens, quarter), bf16),
        pltpu.VMEM((n_ep, tokens, quarter), bf16),
        pltpu.VMEM((n_tp, items, quarter), bf16),
        pltpu.VMEM((items, lanes), f32),
        pltpu.VMEM((n_z, half - 1, 2, sub, units), bf16),
        pltpu.VMEM((n_z, half - 1, 2, sub, units), bf16),
        pltpu.VMEM((n_z, 2, sub, units), f32),
        pltpu.VMEM((items, eg.shape[1]), bf16),
        pltpu.VMEM((2, half, part, quarter), bf16),
        pltpu.VMEM((2, half, part, quarter), bf16),
        pltpu.VMEM((2, half - 1, part, quarter), bf16),
        pltpu.VMEM((2, half - 1, part, quarter), bf16),
        pltpu.VMEM((items, quarter), f32),
        pltpu.VMEM((n_tp, 2, n_z // 2 * sub, units), bf16),
        pltpu.VMEM((2, n_tp, n_z // 2 * sub, quarter), f32),
        pltpu.VMEM((n_z, tokens, quarter), bf16),
        pltpu.VMEM((n_z, tokens, quarter), bf16),
        pltpu.VMEM((n_z - 1, tokens, quarter), bf16),
        pltpu.VMEM((n_z - 1, tokens, quarter), bf16),
        pltpu.SemaphoreType.DMA((6,)),
        pltpu.SemaphoreType.DMA((copies,)),
        pltpu.SemaphoreType.DMA((copies,)),
    ]
    return pl.pallas_call(
        functools.partial(layer_kernel, n_ep, n_tp),
        out_shape=jax.ShapeDtypeStruct((tokens, quarter), bf16),
        in_specs=[vmem] * 6 + [anyspace] * 6,
        out_specs=vmem,
        scratch_shapes=scratch,
        compiler_params=pltpu.CompilerParams(
            collective_id=0, has_side_effects=True, vmem_limit_bytes=60 * 1024 * 1024
        ),
    )(gated, output_weight, hid, gain, gate, sel, eg, eu, ed, dg, du, dd)


def attention_kernel(
    cap,
    hidden_ref,
    gain_ref,
    shift_ref,
    head_gain_ref,
    routes_ref,
    weights_ref,
    qw_hbm,
    kw_hbm,
    vw_hbm,
    ow_hbm,
    fw_hbm,
    state_hbm,
    gated_ref,
    sel_ref,
    new_hbm,
    qw,
    kw,
    vw,
    ow,
    fw,
    state,
    query,
    key,
    value,
    decay,
    readout,
    w_sem,
    in_sem,
    out_sem,
):
    f32, bf16 = jnp.float32, jnp.bfloat16
    tokens = hidden_ref.shape[0]
    heads, key_dim, value_dim = state.shape[1:]
    groups = tokens // 8
    loads = []
    pairs = ((fw_hbm, fw), (kw_hbm, kw), (qw_hbm, qw), (vw_hbm, vw), (ow_hbm, ow))
    for i, (src, dst) in enumerate(pairs):
        load = pltpu.make_async_copy(src, dst, w_sem.at[i])
        load.start()
        loads.append(load)

    def fetch(g):
        rows = pl.ds(g * 8, 8)
        return pltpu.make_async_copy(state_hbm.at[rows], state.at[rows], in_sem.at[g])

    def put(g):
        rows = pl.ds(g * 8, 8)
        return pltpu.make_async_copy(state.at[rows], new_hbm.at[rows], out_sem.at[g])

    for g in range(groups):
        fetch(g).start()

    inputs = hidden_ref[...].astype(f32)
    normed = (inputs * rms_factor(inputs) * flat_row(gain_ref)).astype(bf16)

    items, lanes = sel_ref.shape
    experts = (items // cap + 7) // 8 * 8
    first, second = routes_ref[0:1, :], routes_ref[1:2, :]
    expert = lax.broadcasted_iota(jnp.int32, (experts, tokens), 0)
    chosen0 = jnp.where(expert == first, 1.0, 0.0)
    chosen1 = jnp.where(expert == second, 1.0, 0.0)
    row = lax.broadcasted_iota(jnp.int32, (tokens, tokens), 0)
    col = lax.broadcasted_iota(jnp.int32, (tokens, tokens), 1)
    before = jnp.where(row < col, 1.0, 0.0).astype(bf16)
    earlier = matmul((chosen0 + chosen1).astype(bf16), before)
    slot0 = jnp.sum(earlier * chosen0, axis=0, keepdims=True)
    slot1 = jnp.sum(earlier * chosen1, axis=0, keepdims=True)
    table = lax.broadcasted_iota(jnp.int32, (items, tokens), 0)
    hit0 = table == first * cap + slot0.astype(jnp.int32)
    hit1 = table == second * cap + slot1.astype(jnp.int32)
    comb = jnp.where(hit0, weights_ref[0:1, :], 0.0) + jnp.where(hit1, weights_ref[1:2, :], 0.0)
    weight = jnp.sum(comb, axis=1, keepdims=True)
    weight_hi = weight.astype(bf16).astype(f32)
    lane = lax.broadcasted_iota(jnp.int32, (items, lanes), 1)
    tail = jnp.where(lane == lanes - 2, weight_hi, weight - weight_hi)
    sel_ref[...] = jnp.where(lane < lanes - 2, 0.0, tail).astype(bf16)
    sel_ref[:, :tokens] = (jnp.where(hit0, 1.0, 0.0) + jnp.where(hit1, 1.0, 0.0)).astype(bf16)

    def rounded_rows(weight):
        return matmul(normed, weight[...]).astype(bf16).astype(f32)

    loads[0].wait()
    drive = matmul(normed, fw[...])
    log_sig = jnp.minimum(drive, 0.0) - jnp.log1p(jnp.exp(-jnp.abs(drive)))
    decay[...] = jnp.exp(log_sig / TAU_DECAY + shift_ref[...]).reshape(decay.shape)
    loads[1].wait()
    key[...] = rounded_rows(kw).reshape(key.shape)
    loads[2].wait()
    query[...] = (rounded_rows(qw) * key_dim ** (-0.5)).reshape(query.shape)
    loads[3].wait()
    value[...] = rounded_rows(vw).reshape(value.shape)

    @pl.loop(0, groups)
    def _(g):
        fetch(g).wait()
        for h in range(heads):
            keys = slice(h * key_dim, (h + 1) * key_dim)
            vals = slice(h * value_dim, (h + 1) * value_dim)
            decay_cols = jnp.transpose(decay[g, :, keys])
            key_cols = jnp.transpose(key[g, :, keys])
            query_cols = jnp.transpose(query[g, :, keys])
            for j in range(8):
                fresh = (
                    decay_cols[:, j : j + 1] * state[g * 8 + j, h]
                    + key_cols[:, j : j + 1] * value[g, j : j + 1, vals]
                )
                state[g * 8 + j, h] = fresh
                readout[g, j : j + 1, vals] = jnp.sum(
                    query_cols[:, j : j + 1] * fresh, axis=0, keepdims=True
                )
        put(g).start()

    loads[4].wait()
    outgate = rounded_rows(ow)
    out = readout[...].reshape(tokens, heads * value_dim)
    for h in range(heads):
        vals = slice(h * value_dim, (h + 1) * value_dim)
        part = out[:, vals]
        gain = head_gain_ref[:, vals].astype(f32)
        gated_ref[:, vals] = (part * rms_factor(part) * gain * silu(outgate[:, vals])).astype(bf16)
    for g in range(groups):
        put(g).wait()


def run_attention(hidden, gain, shift, head_gain, routes, weights, qw, kw, vw, ow, fw, state, n_ep):
    bf16, f32 = jnp.bfloat16, jnp.float32
    tokens, heads, key_dim, value_dim = state.shape
    capacity = tokens * routes.shape[0] // n_ep + 2
    cap = (capacity + 15) // 16 * 16
    items = n_ep * cap
    groups = tokens // 8
    lanes = (tokens + 2 + 127) // 128 * 128
    vmem = pl.BlockSpec(memory_space=pltpu.VMEM)
    anyspace = pl.BlockSpec(memory_space=pl.ANY)
    gated, sel, new_state = pl.pallas_call(
        functools.partial(attention_kernel, cap),
        out_shape=(
            jax.ShapeDtypeStruct((tokens, heads * value_dim), bf16),
            jax.ShapeDtypeStruct((items, lanes), bf16),
            jax.ShapeDtypeStruct(state.shape, f32),
        ),
        in_specs=[vmem] * 6 + [anyspace] * 6,
        out_specs=(vmem, vmem, anyspace),
        scratch_shapes=[pltpu.VMEM(w.shape, bf16) for w in (qw, kw, vw, ow, fw)]
        + [
            pltpu.VMEM(state.shape, f32),
            pltpu.VMEM((groups, 8, heads * key_dim), f32),
            pltpu.VMEM((groups, 8, heads * key_dim), f32),
            pltpu.VMEM((groups, 8, heads * value_dim), f32),
            pltpu.VMEM((groups, 8, heads * key_dim), f32),
            pltpu.VMEM((groups, 8, heads * value_dim), f32),
            pltpu.SemaphoreType.DMA((5,)),
            pltpu.SemaphoreType.DMA((groups,)),
            pltpu.SemaphoreType.DMA((groups,)),
        ],
        compiler_params=pltpu.CompilerParams(vmem_limit_bytes=60 * 1024 * 1024),
    )(hidden, gain, shift, head_gain, routes, weights, qw, kw, vw, ow, fw, state)
    return gated, sel.reshape(n_ep, cap, lanes), new_state


def body(
    hidden_in,
    carried_state,
    input_gain,
    query_weight,
    key_weight,
    value_weight,
    outgate_weight,
    decay_weight,
    decay_shift,
    head_gain,
    output_weight,
    channel_gain,
    branch_gate,
    routes,
    route_weights,
    expert_gate,
    expert_up,
    expert_down,
    dense_gate,
    dense_up,
    dense_down,
):
    gated, sel, new_state = run_attention(
        hidden_in,
        input_gain.reshape(-1, 128),
        decay_shift,
        head_gain.reshape(1, -1),
        routes.T,
        route_weights.T,
        query_weight,
        key_weight,
        value_weight,
        outgate_weight,
        decay_weight,
        carried_state,
        lax.axis_size("ep"),
    )
    mixed = run_layer(
        gated,
        output_weight,
        hidden_in,
        channel_gain.reshape(-1, 128),
        branch_gate.reshape(-1, 128),
        sel,
        expert_gate[0],
        expert_up[0],
        expert_down[0],
        dense_gate,
        dense_up,
        dense_down,
    )
    return (mixed, new_state)


def solution(mesh):
    in_specs = (
        P("ep", None),
        P("ep", "tp", None, None),
        P(),
        P(None, "tp"),
        P(None, "tp"),
        P(None, "tp"),
        P(None, "tp"),
        P(None, "tp"),
        P("ep", "tp"),
        P("tp", None),
        P("tp", None),
        P(),
        P(),
        P("ep", None),
        P("ep", None),
        P("ep", None, "tp"),
        P("ep", None, "tp"),
        P("ep", "tp", None),
        P("tp", "ep"),
        P("tp", "ep"),
        P("ep", "tp"),
    )
    out_specs = (P("ep", "tp"), P("ep", "tp", None, None))
    return jax.shard_map(body, mesh=mesh, in_specs=in_specs, out_specs=out_specs, check_vma=False)
```

```python
import functools

import jax
import jax.numpy as jnp
from jax import lax
from jax.experimental import pallas as pl
from jax.experimental.pallas import tpu as pltpu
from jax.sharding import PartitionSpec as P

EPSILON = 1e-06
TAU_DECAY = 16.0
MESH = pl.DeviceIdType.MESH


def rms_factor(values):
    return lax.rsqrt(jnp.mean(values * values, axis=-1, keepdims=True) + EPSILON)


def matmul(left, right):
    return jnp.dot(left, right, preferred_element_type=jnp.float32)


def flat_row(ref):
    rows = ref[...].astype(jnp.float32)
    return jnp.concatenate([rows[k : k + 1, :] for k in range(rows.shape[0])], axis=1)


def in_hbm(array):
    return pltpu.with_memory_space_constraint(array, pltpu.HBM)


def silu(values):
    return values * jax.nn.sigmoid(values)


def layer_kernel(
    n_ep,
    n_tp,
    gated_ref,
    outw_ref,
    hid_ref,
    gain_ref,
    gate_ref,
    sel_ref,
    eg_hbm,
    eu_hbm,
    ed_hbm,
    dg_hbm,
    du_hbm,
    dd_hbm,
    mixed_ref,
    eg,
    eu,
    ed,
    wg,
    wu,
    ddw,
    gain_row,
    gate_row,
    sel_recv,
    p_send,
    p_recv,
    stat,
    scale_rows,
    mid_buf,
    piece,
    other,
    rows_all,
    row_scale,
    gu_send,
    gu_recv,
    gu_own,
    e_hid,
    near_send,
    near_recv,
    far_send,
    far_recv,
    eo_own,
    d_hid,
    d_out,
    y_send,
    y_recv,
    z_send,
    z_recv,
    w_sem,
    ssem,
    rsem,
):
    f32, bf16 = jnp.float32, jnp.bfloat16
    ep = lax.axis_index("ep")
    tp = lax.axis_index("tp")
    tokens, width = hid_ref.shape
    quarter = width // n_tp
    cap, lanes = sel_ref.shape[1:]
    units = dg_hbm.shape[1]
    n_z, half = n_ep // 2, n_tp // 2
    h, c = lax.div(tp, 2), lax.rem(tp, 2)
    partner = tp + 1 - 2 * c
    near = ep + 1 - 2 * lax.rem(ep, 2)
    steps = [0] + sorted(range(1, n_z), key=lambda m: abs(m - n_z // 2))
    own = pl.ds(pl.multiple_of(tp * quarter, quarter), quarter)

    def columns(q):
        return pl.ds(pl.multiple_of(q * quarter, quarter), quarter)

    def member(t, r):
        return lax.rem((near if r else ep) - 2 * steps[t] + n_ep, n_ep)

    def peer(dh, dc):
        return lax.rem(h + dh, half) * 2 + lax.rem(c + dc, 2)

    loads = []
    pairs = ((dg_hbm, wg.at[c]), (du_hbm, wu.at[c]), (eg_hbm, eg), (eu_hbm, eu))
    for i, (src, dst) in enumerate(pairs + ((ed_hbm, ed), (dd_hbm, ddw))):
        load = pltpu.make_async_copy(src, dst, w_sem.at[i])
        load.start()
        loads.append(load)

    gain_row[...] = flat_row(gain_ref)
    gate_row[...] = flat_row(gate_ref)
    barrier = pltpu.get_barrier_semaphore()
    for d in range(1, n_tp):
        pl.semaphore_signal(
            barrier, inc=1, device_id=(ep, lax.rem(tp + d, n_tp)), device_id_type=MESH
        )
    for d in range(1, n_ep):
        pl.semaphore_signal(
            barrier, inc=1, device_id=(lax.rem(ep + d, n_ep), tp), device_id_type=MESH
        )

    sent = []

    def send(src, dst, device):
        copy = pltpu.make_async_remote_copy(
            src_ref=src,
            dst_ref=dst,
            send_sem=ssem.at[len(sent)],
            recv_sem=rsem.at[len(sent)],
            device_id=device,
            device_id_type=MESH,
        )
        copy.start()
        sent.append(copy)
        return copy

    peers = [(dh, dc) for dh in range(1, half) for dc in range(2)] + [(0, 1)]
    for i, (dh, dc) in enumerate(peers):
        part = matmul(gated_ref[...], outw_ref[:, columns(peer(dh, dc))])
        p_send[i] = part.astype(bf16)
    pl.semaphore_wait(barrier, n_tp + n_ep - 2)
    c_part = []
    for i, (dh, dc) in enumerate(peers):
        c_part.append(send(p_send.at[i], p_recv.at[i], (ep, peer(dh, dc))))
    c_sel = []
    for d in range(1, n_ep):
        target = lax.rem(ep + d, n_ep)
        c_sel.append(send(sel_ref.at[target], sel_recv.at[ep], (target, tp)))
    c_dense = [
        send(dg_hbm, wg.at[c], (ep, partner)),
        send(du_hbm, wu.at[c], (ep, partner)),
    ]
    sel_recv[ep] = sel_ref[ep]
    attended = matmul(gated_ref[...], outw_ref[:, own]).astype(bf16).astype(f32)
    for i in reversed(range(len(peers))):
        c_part[i].wait_recv()
        attended = attended + p_recv[i].astype(f32)
    middle = (hid_ref[:, own].astype(f32) + attended).astype(bf16).astype(f32)
    shaped = middle * gain_row[:, own]
    piece[ep] = shaped.astype(bf16)
    squares = jnp.sum(middle * middle, axis=-1, keepdims=True)
    inner = jnp.sum(shaped * gate_row[:, own], axis=-1, keepdims=True)
    line = lax.broadcasted_iota(jnp.int32, (tokens, lanes), 0)
    lane = lax.broadcasted_iota(jnp.int32, (tokens, lanes), 1)
    eye = jnp.where(line == lane, 1.0, 0.0)
    stat[tp, ep, 0:1, :] = jnp.sum(eye * squares, axis=0, keepdims=True)
    stat[tp, ep, 1:2, :] = jnp.sum(eye * inner, axis=0, keepdims=True)
    c_near = send(piece.at[ep], piece.at[ep], (near, tp))
    c_stat = []
    for d in range(1, n_ep):
        target = lax.rem(ep + d, n_ep)
        c_stat.append(send(stat.at[tp, ep], stat.at[tp, ep], (target, tp)))
    c_z = [None]
    for t in range(1, n_z):
        target = lax.rem(ep + 2 * steps[t], n_ep)
        c_z.append(send(piece.at[ep], piece.at[ep], (target, tp)))
    mid_buf[...] = middle

    c_other = {}

    def share(t, r):
        block = member(t, r)
        c_other[t, r] = send(piece.at[block], other.at[block], (ep, partner))

    def pick(q, t, r, source):
        block = member(t, r)
        picked = matmul(sel_recv[block][:, :tokens], source[block]).astype(bf16)
        rows_all[q, (2 * t + r) * cap : (2 * t + r + 1) * cap, :] = picked

    c_rows, c_pass, c_gu, c_hid, c_hid_near = {}, {}, {}, {}, {}
    c_eo_near, c_eo_far, c_y, c_out = {}, {}, {}, {}
    sub = tokens // half
    per_part = n_z // 2
    parts = [range(p * per_part, (p + 1) * per_part) for p in range(2)]

    def of_chip(value, index):
        chosen = value[:sub]
        for k in range(1, half):
            chosen = jnp.where(index == k, value[k * sub : (k + 1) * sub], chosen)
        return chosen

    def span_of(t):
        return pl.ds(2 * t * cap, 2 * cap)

    def send_rows(t):
        for dh in range(1, half):
            rows = rows_all.at[tp, span_of(t)]
            c_rows[t, dh] = send(rows, rows, (ep, peer(dh, 0)))

    def pass_rows(t):
        for dh in range(1, half):
            c_rows[t, dh].wait_recv()
            q = lax.rem(h - dh + half, half) * 2 + c
            rows = rows_all.at[q, span_of(t)]
            c_pass[t, dh] = send(rows, rows, (ep, partner))

    def partial(t):
        for r in range(2):
            c_other[t, r].wait_recv()
        block = lax.rem(jnp.where(c == 1, near, ep) - 2 * steps[t] + n_ep, n_ep)
        left, right = piece[block], other[block]
        for i, w in enumerate((wg, wu)):
            product = matmul(left, w[c]) + matmul(right, w[1 - c])
            gu_own[t, i] = of_chip(product, h)
            for dh in range(1, half):
                gu_send[t, dh - 1, i] = of_chip(product, lax.rem(h + dh, half)).astype(bf16)
        for dh in range(1, half):
            source, target = gu_send.at[t, dh - 1], gu_recv.at[t, dh - 1]
            c_gu[t, dh] = send(source, target, (ep, peer(dh, 0)))

    line_own = lax.broadcasted_iota(jnp.int32, (sub, lanes), 0) + h * sub
    eye_own = jnp.where(line_own == lax.broadcasted_iota(jnp.int32, (sub, lanes), 1), 1.0, 0.0)

    def activate(p):
        shares = []
        for t in parts[p]:
            gate_sum, up_sum = gu_own[t, 0], gu_own[t, 1]
            for dh in range(1, half):
                c_gu[t, dh].wait_recv()
                gate_sum = gate_sum + gu_recv[t, dh - 1, 0].astype(f32)
                up_sum = up_sum + gu_recv[t, dh - 1, 1].astype(f32)
            block = lax.rem(jnp.where(c == 1, near, ep) - 2 * steps[t] + n_ep, n_ep)
            scale = jnp.sum(eye_own * scale_rows[block, 0:1, :], axis=1, keepdims=True)
            shares.append(silu(gate_sum * scale) * (up_sum * scale))
        d_hid[tp, p] = jnp.concatenate(shares, axis=0).astype(bf16)
        mine = d_hid.at[tp, p]
        for dh in range(1, half):
            c_hid[p, dh] = send(mine, mine, (ep, peer(dh, 0)))
        c_hid_near[p, 0] = send(mine, mine, (ep, partner))

    def pass_hidden(p):
        for dh in range(1, half):
            c_hid[p, dh].wait_recv()
            got = d_hid.at[lax.rem(h - dh + half, half) * 2 + c, p]
            c_hid_near[p, dh] = send(got, got, (ep, partner))

    def dense_down(p):
        for dh in range(half):
            c_hid_near[p, dh].wait_recv()
        hidden = d_hid[:, p].reshape(n_tp * per_part * sub, units)
        d_out[p] = matmul(hidden, ddw[...]).reshape(d_out.shape[1:])

    def scales():
        for copy in c_total:
            copy.wait_recv()
        totals = stat[0]
        for q in range(1, n_tp):
            totals = totals + stat[q]
        factors = lax.rsqrt(totals[:, 0:1, :] / width + EPSILON)
        scale_rows[:, 0:1, :] = factors
        scale_rows[:, 1:2, :] = jax.nn.sigmoid(totals[:, 1:2, :] * factors)

    count = 2 * per_part * cap
    chosen_lane = lax.broadcasted_iota(jnp.int32, (cap, lanes), 1)

    def prepare(p):
        for t in parts[p]:
            for r in range(2):
                pick(partner, t, r, other)
                block = member(t, r)
                chosen = sel_recv[block].astype(f32)
                masked = jnp.where(chosen_lane < tokens, chosen * scale_rows[block, 0:1, :], 0.0)
                column = jnp.sum(masked, axis=1, keepdims=True)
                at = slice((2 * t + r) * cap, (2 * t + r + 1) * cap)
                row_scale[at, :] = jnp.broadcast_to(column, (cap, lanes))

    inner_width = eg.shape[1]
    tile = 256 if inner_width % 256 == 0 else 128

    def expert_in(p):
        for t in parts[p]:
            for dh in range(1, half):
                c_pass[t, dh].wait_recv()
        at = slice(p * count, (p + 1) * count)

        scale = row_scale[at, 0:1]
        for i in range(inner_width // tile):
            cols = slice(i * tile, (i + 1) * tile)
            gate_part = matmul(rows_all[0, at], eg[0:quarter, cols])
            up_part = matmul(rows_all[0, at], eu[0:quarter, cols])
            for q in range(1, n_tp):
                span = slice(q * quarter, (q + 1) * quarter)
                gate_part = gate_part + matmul(rows_all[q, at], eg[span, cols])
                up_part = up_part + matmul(rows_all[q, at], eu[span, cols])
            e_hid[at, cols] = (silu(gate_part * scale) * (up_part * scale)).astype(bf16)

    def expert_near(p):
        at = slice(p * count, (p + 1) * count)
        for i, dh in enumerate(list(range(1, half)) + [0]):
            near_send[p, i] = matmul(e_hid[at, :], ed[:, columns(peer(dh, 1))]).astype(bf16)
            source, target = near_send.at[p, i], near_recv.at[p, i]
            c_eo_near[p, i] = send(source, target, (ep, partner))

    def expert_far(p):
        at = slice(p * count, (p + 1) * count)
        for i, dh in enumerate(range(1, half)):
            part = matmul(e_hid[at, :], ed[:, columns(peer(dh, 0))])
            c_eo_near[p, i].wait_recv()
            far_send[p, i] = (part + near_recv[p, i].astype(f32)).astype(bf16)
            source, target = far_send.at[p, i], far_recv.at[p, i]
            c_eo_far[p, i] = send(source, target, (ep, peer(dh, 0)))
        part = matmul(e_hid[at, :], ed[:, own])
        c_eo_near[p, half - 1].wait_recv()
        eo_own[at, :] = part + near_recv[p, half - 1].astype(f32)

    def expert_total(p):
        at = slice(p * count, (p + 1) * count)
        total = eo_own[at, :]
        for i in range(half - 1):
            c_eo_far[p, i].wait_recv()
            total = total + far_recv[p, i].astype(f32)
        eo_own[at, :] = total

    def outcome(t, r):
        block = member(t, r)
        span = slice((2 * t + r) * cap, (2 * t + r + 1) * cap)
        chosen = sel_recv[block]
        weight = chosen[:, lanes - 2 : lanes - 1].astype(f32)
        weight = weight + chosen[:, lanes - 1 : lanes].astype(f32)
        answers = (eo_own[span, :] * weight).astype(bf16)
        routed = lax.dot_general(
            chosen[:, :tokens], answers, (((0,), (0,)), ((), ())), preferred_element_type=f32
        )
        branch = jnp.sum(eye * scale_rows[block, 1:2, :], axis=1, keepdims=True)
        p, k = t // per_part, t % per_part
        dense = [d_out[p, 2 * j + r, k * sub : (k + 1) * sub, :] for j in range(half)]
        return branch * jnp.concatenate(dense, axis=0) + routed

    def far_first(p):
        return [t for t in parts[p] if t] + [t for t in parts[p] if not t]

    def send_near(p):
        for t in far_first(p):
            y_send[t] = outcome(t, 1).astype(bf16)
            c_y[t] = send(y_send.at[t], y_recv.at[t], (near, tp))

    def send_out(p):
        for t in far_first(p):
            mine = outcome(t, 0)
            c_y[t].wait_recv()
            mine = mine + y_recv[t].astype(f32)
            if t:
                z_send[t - 1] = mine.astype(bf16)
                c_out[t] = send(z_send.at[t - 1], z_recv.at[t - 1], (member(t, 0), tp))
            else:
                mid_buf[...] = mid_buf[...] + mine

    share(0, 0)
    for copy in c_sel:
        copy.wait_recv()
    pick(tp, 0, 0, piece)
    c_near.wait_recv()
    share(0, 1)
    pick(tp, 0, 1, piece)
    send_rows(0)
    c_relay = [None]
    for t in range(1, n_z):
        c_z[t].wait_recv()
        block = member(t, 0)
        c_relay.append(send(piece.at[block], piece.at[block], (near, tp)))
        share(t, 0)
        pick(tp, t, 0, piece)
        if t == 1:
            loads[0].wait()
            loads[1].wait()
            for copy in c_dense:
                copy.wait_recv()
            partial(0)
    for copy in c_stat:
        copy.wait_recv()
    c_total = []
    for dh, dc in peers:
        c_total.append(send(stat.at[tp], stat.at[tp], (ep, peer(dh, dc))))
    for t in range(1, n_z):
        c_relay[t].wait_recv()
        share(t, 1)
        pick(tp, t, 1, piece)
        send_rows(t)
        if t > 1:
            partial(t - 1)
        if t != 2:
            pass_rows(max(t - 2, 0))
    scales()
    prepare(0)
    for t in range(max(n_z - 2, 1), per_part):
        pass_rows(t)
    partial(n_z - 1)
    loads[2].wait()
    loads[3].wait()
    expert_in(0)
    for t in range(max(n_z - 2, per_part), n_z):
        pass_rows(t)
    loads[4].wait()
    expert_near(0)
    activate(0)
    prepare(1)
    expert_far(0)
    activate(1)
    expert_in(1)
    expert_near(1)
    pass_hidden(0)
    expert_far(1)
    loads[5].wait()
    dense_down(0)
    expert_total(0)
    send_near(0)
    pass_hidden(1)
    dense_down(1)
    expert_total(1)
    send_near(1)
    send_out(0)
    send_out(1)
    mine = mid_buf[...]
    for t in range(1, n_z):
        c_out[t].wait_recv()
        mine = mine + z_recv[t - 1].astype(f32)
    mixed_ref[...] = mine.astype(bf16)
    for copy in sent:
        copy.wait_send()


def run_layer(gated, output_weight, hid, gain, gate, sel, eg, eu, ed, dg, du, dd):
    n_ep, n_tp = lax.axis_size("ep"), lax.axis_size("tp")
    tokens = hid.shape[0]
    quarter = hid.shape[1] // n_tp
    cap, lanes = sel.shape[1:]
    items = n_ep * cap
    n_z, half = n_ep // 2, n_tp // 2
    sub = tokens // half
    part = items // 2
    units = dg.shape[1]
    bf16, f32 = jnp.bfloat16, jnp.float32
    vmem = pl.BlockSpec(memory_space=pltpu.VMEM)
    anyspace = pl.BlockSpec(memory_space=pl.ANY)
    copies = 8 * n_ep + 4 * n_tp + 6 * n_z + 16
    scratch = [pltpu.VMEM(w.shape, bf16) for w in (eg, eu, ed)]
    scratch += [
        pltpu.VMEM((2, quarter, units), bf16),
        pltpu.VMEM((2, quarter, units), bf16),
        pltpu.VMEM(dd.shape, bf16),
        pltpu.VMEM((1, hid.shape[1]), f32),
        pltpu.VMEM((1, hid.shape[1]), f32),
        pltpu.VMEM(sel.shape, bf16),
        pltpu.VMEM((n_tp - 1, tokens, quarter), bf16),
        pltpu.VMEM((n_tp - 1, tokens, quarter), bf16),
        pltpu.VMEM((n_tp, n_ep, 2, lanes), f32),
        pltpu.VMEM((n_ep, 2, lanes), f32),
        pltpu.VMEM((tokens, quarter), f32),
        pltpu.VMEM((n_ep, tokens, quarter), bf16),
        pltpu.VMEM((n_ep, tokens, quarter), bf16),
        pltpu.VMEM((n_tp, items, quarter), bf16),
        pltpu.VMEM((items, lanes), f32),
        pltpu.VMEM((n_z, half - 1, 2, sub, units), bf16),
        pltpu.VMEM((n_z, half - 1, 2, sub, units), bf16),
        pltpu.VMEM((n_z, 2, sub, units), f32),
        pltpu.VMEM((items, eg.shape[1]), bf16),
        pltpu.VMEM((2, half, part, quarter), bf16),
        pltpu.VMEM((2, half, part, quarter), bf16),
        pltpu.VMEM((2, half - 1, part, quarter), bf16),
        pltpu.VMEM((2, half - 1, part, quarter), bf16),
        pltpu.VMEM((items, quarter), f32),
        pltpu.VMEM((n_tp, 2, n_z // 2 * sub, units), bf16),
        pltpu.VMEM((2, n_tp, n_z // 2 * sub, quarter), f32),
        pltpu.VMEM((n_z, tokens, quarter), bf16),
        pltpu.VMEM((n_z, tokens, quarter), bf16),
        pltpu.VMEM((n_z - 1, tokens, quarter), bf16),
        pltpu.VMEM((n_z - 1, tokens, quarter), bf16),
        pltpu.SemaphoreType.DMA((6,)),
        pltpu.SemaphoreType.DMA((copies,)),
        pltpu.SemaphoreType.DMA((copies,)),
    ]
    return pl.pallas_call(
        functools.partial(layer_kernel, n_ep, n_tp),
        out_shape=jax.ShapeDtypeStruct((tokens, quarter), bf16),
        in_specs=[vmem] * 6 + [anyspace] * 6,
        out_specs=vmem,
        scratch_shapes=scratch,
        compiler_params=pltpu.CompilerParams(
            collective_id=0, has_side_effects=True, vmem_limit_bytes=36 * 1024 * 1024
        ),
    )(gated, output_weight, hid, gain, gate, sel, *map(in_hbm, (eg, eu, ed, dg, du, dd)))


def attention_kernel(
    cap,
    hidden_hbm,
    gain_hbm,
    shift_hbm,
    head_gain_hbm,
    routes_hbm,
    weights_hbm,
    qw_hbm,
    kw_hbm,
    vw_hbm,
    ow_hbm,
    fw_hbm,
    state_hbm,
    outw_hbm,
    gated_ref,
    sel_ref,
    hidden_ref,
    outw_ref,
    new_hbm,
    gain_ref,
    shift_ref,
    head_gain_ref,
    routes_ref,
    weights_ref,
    qw,
    kw,
    vw,
    ow,
    fw,
    state,
    key_query,
    value,
    decay,
    readout,
    w_sem,
    in_sem,
    out_sem,
):
    f32, bf16 = jnp.float32, jnp.bfloat16
    tokens = hidden_hbm.shape[0]
    heads, key_dim, value_dim = state.shape[1:]
    groups = tokens // 8
    loads = []
    pairs = (
        (fw_hbm, fw),
        (kw_hbm, kw),
        (qw_hbm, qw),
        (vw_hbm, vw),
        (ow_hbm, ow),
        (hidden_hbm, hidden_ref),
        (gain_hbm, gain_ref),
        (routes_hbm, routes_ref),
        (weights_hbm, weights_ref),
        (shift_hbm, shift_ref),
        (head_gain_hbm, head_gain_ref),
        (outw_hbm, outw_ref),
    )
    for i, (src, dst) in enumerate(pairs):
        loads.append(pltpu.make_async_copy(src, dst, w_sem.at[i]))
    for i in (5, 6, 0, 1, 2, 3, 7, 8, 9, 10):
        loads[i].start()

    def fetch(g):
        rows = pl.ds(g * 8, 8)
        return pltpu.make_async_copy(state_hbm.at[rows], state.at[rows], in_sem.at[g])

    def put(g):
        rows = pl.ds(g * 8, 8)
        return pltpu.make_async_copy(state.at[rows], new_hbm.at[rows], out_sem.at[g])

    loads[5].wait()
    for g in range(groups):
        fetch(g).start()
    loads[4].start()
    loads[11].start()
    loads[6].wait()
    inputs = hidden_ref[...].astype(f32)
    normed = (inputs * rms_factor(inputs) * flat_row(gain_ref)).astype(bf16)

    loads[7].wait()
    loads[8].wait()
    items, lanes = sel_ref.shape
    experts = (items // cap + 7) // 8 * 8
    first, second = routes_ref[0:1, :], routes_ref[1:2, :]
    expert = lax.broadcasted_iota(jnp.int32, (experts, tokens), 0)
    chosen0 = jnp.where(expert == first, 1.0, 0.0)
    chosen1 = jnp.where(expert == second, 1.0, 0.0)
    row = lax.broadcasted_iota(jnp.int32, (tokens, tokens), 0)
    col = lax.broadcasted_iota(jnp.int32, (tokens, tokens), 1)
    before = jnp.where(row < col, 1.0, 0.0).astype(bf16)
    earlier = matmul((chosen0 + chosen1).astype(bf16), before)
    slot0 = jnp.sum(earlier * chosen0, axis=0, keepdims=True)
    slot1 = jnp.sum(earlier * chosen1, axis=0, keepdims=True)
    table = lax.broadcasted_iota(jnp.int32, (items, tokens), 0)
    hit0 = table == first * cap + slot0.astype(jnp.int32)
    hit1 = table == second * cap + slot1.astype(jnp.int32)
    comb = jnp.where(hit0, weights_ref[0:1, :], 0.0) + jnp.where(hit1, weights_ref[1:2, :], 0.0)
    weight = jnp.sum(comb, axis=1, keepdims=True)
    weight_hi = weight.astype(bf16).astype(f32)
    lane = lax.broadcasted_iota(jnp.int32, (items, lanes), 1)
    tail = jnp.where(lane == lanes - 2, weight_hi, weight - weight_hi)
    sel_ref[...] = jnp.where(lane < lanes - 2, 0.0, tail).astype(bf16)
    sel_ref[:, :tokens] = (jnp.where(hit0, 1.0, 0.0) + jnp.where(hit1, 1.0, 0.0)).astype(bf16)

    def rounded_rows(weight):
        return matmul(normed, weight[...]).astype(bf16).astype(f32)

    loads[0].wait()
    loads[9].wait()
    loads[10].wait()
    drive = matmul(normed, fw[...])
    log_sig = jnp.minimum(drive, 0.0) - jnp.log1p(jnp.exp(-jnp.abs(drive)))
    decay[...] = jnp.exp(log_sig / TAU_DECAY + shift_ref[...]).reshape(decay.shape)
    loads[1].wait()
    key_query[:, 0:8] = rounded_rows(kw).reshape(decay.shape)
    loads[2].wait()
    key_query[:, 8:16] = rounded_rows(qw).reshape(decay.shape)
    loads[3].wait()
    value[...] = rounded_rows(vw).reshape(value.shape)
    spread_width = value_dim + 128
    token = lax.broadcasted_iota(jnp.int32, (16, spread_width), 0)
    column = lax.broadcasted_iota(jnp.int32, (16, spread_width), 1)
    unit = jnp.ones((1, 128), f32)

    @pl.loop(0, groups)
    def _(g):
        fetch(g).wait()
        for h in range(heads):
            keys = slice(h * key_dim, (h + 1) * key_dim)
            vals = slice(h * value_dim, (h + 1) * value_dim)
            decay_cols = jnp.transpose(decay[g, :, keys])
            left = jnp.transpose(key_query[g, :, keys]).astype(bf16)
            for j in range(8):
                right = jnp.concatenate([value[g, j : j + 1, vals], unit], axis=1)
                wanted = token == jnp.where(column < value_dim, j, 8 + j)
                products = matmul(left, jnp.where(wanted, right, 0.0).astype(bf16))
                fresh = decay_cols[:, j : j + 1] * state[g * 8 + j, h] + products[:, :value_dim]
                state[g * 8 + j, h] = fresh
                asked = products[:, value_dim:]
                asked = jnp.concatenate([asked] * (value_dim // 128), axis=1)
                readout[g, j : j + 1, vals] = jnp.sum(asked * fresh, axis=0, keepdims=True)
        put(g).start()

    loads[4].wait()
    outgate = rounded_rows(ow)
    out = readout[...].reshape(tokens, heads * value_dim) * key_dim ** (-0.5)
    for h in range(heads):
        vals = slice(h * value_dim, (h + 1) * value_dim)
        part = out[:, vals]
        gain = head_gain_ref[:, vals].astype(f32)
        gated_ref[:, vals] = (part * rms_factor(part) * gain * silu(outgate[:, vals])).astype(bf16)
    loads[11].wait()
    for g in range(groups):
        put(g).wait()


def run_attention(
    hidden, gain, shift, head_gain, routes, weights, qw, kw, vw, ow, fw, state, outw, n_ep
):
    bf16, f32 = jnp.bfloat16, jnp.float32
    tokens, heads, key_dim, value_dim = state.shape
    capacity = tokens * routes.shape[0] // n_ep + 2
    cap = (capacity + 15) // 16 * 16
    items = n_ep * cap
    groups = tokens // 8
    lanes = (tokens + 2 + 127) // 128 * 128
    vmem = pl.BlockSpec(memory_space=pltpu.VMEM)
    anyspace = pl.BlockSpec(memory_space=pl.ANY)
    operands = (hidden, gain, shift, head_gain, routes, weights, qw, kw, vw, ow, fw, state, outw)
    gated, sel, hidden, outw, new_state = pl.pallas_call(
        functools.partial(attention_kernel, cap),
        out_shape=(
            pltpu.VMEM((tokens, heads * value_dim), bf16),
            pltpu.VMEM((items, lanes), bf16),
            pltpu.VMEM(hidden.shape, bf16),
            pltpu.VMEM(outw.shape, bf16),
            jax.ShapeDtypeStruct(state.shape, f32),
        ),
        in_specs=[anyspace] * 13,
        out_specs=(vmem, vmem, vmem, vmem, anyspace),
        scratch_shapes=[pltpu.VMEM(a.shape, a.dtype) for a in operands[1:11]]
        + [
            pltpu.VMEM(state.shape, f32),
            pltpu.VMEM((groups, 16, heads * key_dim), f32),
            pltpu.VMEM((groups, 8, heads * value_dim), f32),
            pltpu.VMEM((groups, 8, heads * key_dim), f32),
            pltpu.VMEM((groups, 8, heads * value_dim), f32),
            pltpu.SemaphoreType.DMA((12,)),
            pltpu.SemaphoreType.DMA((groups,)),
            pltpu.SemaphoreType.DMA((groups,)),
        ],
        compiler_params=pltpu.CompilerParams(vmem_limit_bytes=24 * 1024 * 1024),
    )(*map(in_hbm, operands))
    return gated, sel.reshape(n_ep, cap, lanes), hidden, outw, new_state


def body(
    hidden_in,
    carried_state,
    input_gain,
    query_weight,
    key_weight,
    value_weight,
    outgate_weight,
    decay_weight,
    decay_shift,
    head_gain,
    output_weight,
    channel_gain,
    branch_gate,
    routes,
    route_weights,
    expert_gate,
    expert_up,
    expert_down,
    dense_gate,
    dense_up,
    dense_down,
):
    gated, sel, hidden, outw, new_state = run_attention(
        hidden_in,
        input_gain.reshape(-1, 128),
        decay_shift,
        head_gain.reshape(1, -1),
        routes.T,
        route_weights.T,
        query_weight,
        key_weight,
        value_weight,
        outgate_weight,
        decay_weight,
        carried_state,
        output_weight,
        lax.axis_size("ep"),
    )
    mixed = run_layer(
        gated,
        outw,
        hidden,
        channel_gain.reshape(-1, 128),
        branch_gate.reshape(-1, 128),
        sel,
        expert_gate[0],
        expert_up[0],
        expert_down[0],
        dense_gate,
        dense_up,
        dense_down,
    )
    return (mixed, new_state)


def solution(mesh):
    in_specs = (
        P("ep", None),
        P("ep", "tp", None, None),
        P(),
        P(None, "tp"),
        P(None, "tp"),
        P(None, "tp"),
        P(None, "tp"),
        P(None, "tp"),
        P("ep", "tp"),
        P("tp", None),
        P("tp", None),
        P(),
        P(),
        P("ep", None),
        P("ep", None),
        P("ep", None, "tp"),
        P("ep", None, "tp"),
        P("ep", "tp", None),
        P("tp", "ep"),
        P("tp", "ep"),
        P("ep", "tp"),
    )
    out_specs = (P("ep", "tp"), P("ep", "tp", None, None))
    return jax.shard_map(body, mesh=mesh, in_specs=in_specs, out_specs=out_specs, check_vma=False)
```

```python
import functools

import jax
import jax.numpy as jnp
from jax import lax
from jax.experimental import pallas as pl
from jax.experimental.pallas import tpu as pltpu
from jax.sharding import PartitionSpec as P

EPSILON = 1e-06
TAU_DECAY = 16.0
MESH = pl.DeviceIdType.MESH


def rms_factor(values):
    return lax.rsqrt(jnp.mean(values * values, axis=-1, keepdims=True) + EPSILON)


def matmul(left, right):
    return jnp.dot(left, right, preferred_element_type=jnp.float32)


def flat_row(ref):
    rows = ref[...].astype(jnp.float32)
    return jnp.concatenate([rows[k : k + 1, :] for k in range(rows.shape[0])], axis=1)


def in_hbm(array):
    return pltpu.with_memory_space_constraint(array, pltpu.HBM)


def silu(values):
    return values * jax.nn.sigmoid(values)


def layer_kernel(
    n_ep,
    n_tp,
    gated_ref,
    outw_ref,
    hid_ref,
    gain_ref,
    gate_ref,
    sel_ref,
    eg_hbm,
    eu_hbm,
    ed_hbm,
    dg_hbm,
    du_hbm,
    dd_hbm,
    mixed_ref,
    eg,
    eu,
    ed,
    wg,
    wu,
    ddw,
    gain_row,
    gate_row,
    sel_recv,
    p_send,
    p_recv,
    stat,
    scale_rows,
    mid_buf,
    piece,
    other,
    rows_all,
    row_scale,
    gu_send,
    gu_recv,
    gu_own,
    e_hid,
    near_send,
    near_recv,
    far_send,
    far_recv,
    eo_own,
    d_hid,
    d_out,
    y_send,
    y_recv,
    z_send,
    z_recv,
    w_sem,
    ssem,
    rsem,
):
    f32, bf16 = jnp.float32, jnp.bfloat16
    ep = lax.axis_index("ep")
    tp = lax.axis_index("tp")
    tokens, width = hid_ref.shape
    quarter = width // n_tp
    cap, lanes = sel_ref.shape[1:]
    units = dg_hbm.shape[1]
    n_z, half = n_ep // 2, n_tp // 2
    h, c = lax.div(tp, 2), lax.rem(tp, 2)
    partner = tp + 1 - 2 * c
    near = ep + 1 - 2 * lax.rem(ep, 2)
    steps = list(range(n_z))
    mirrored = n_z & (n_z - 1) == 0
    own = pl.ds(pl.multiple_of(tp * quarter, quarter), quarter)

    def columns(q):
        return pl.ds(pl.multiple_of(q * quarter, quarter), quarter)

    def member(t, r, ahead=False):
        base, step = near if r else ep, steps[t]
        if not mirrored:
            return lax.rem(base + (2 * step if ahead else n_ep - 2 * step), n_ep)
        target, bit = lax.rem(base, 2), 1
        while bit < n_z:
            digit = lax.rem(lax.div(base, 2 * bit), 2)
            target = target + 2 * bit * (1 - digit if step & bit else digit)
            bit *= 2
        return target

    def peer(dh, dc):
        return lax.rem(h + dh, half) * 2 + lax.rem(c + dc, 2)

    loads = []
    pairs = ((dg_hbm, wg.at[c]), (du_hbm, wu.at[c]), (eg_hbm, eg), (eu_hbm, eu))
    for i, (src, dst) in enumerate(pairs + ((ed_hbm, ed), (dd_hbm, ddw))):
        load = pltpu.make_async_copy(src, dst, w_sem.at[i])
        load.start()
        loads.append(load)

    gain_row[...] = flat_row(gain_ref)
    gate_row[...] = flat_row(gate_ref)
    barrier = pltpu.get_barrier_semaphore()
    for d in range(1, n_tp):
        pl.semaphore_signal(
            barrier, inc=1, device_id=(ep, lax.rem(tp + d, n_tp)), device_id_type=MESH
        )
    for d in range(1, n_ep):
        pl.semaphore_signal(
            barrier, inc=1, device_id=(lax.rem(ep + d, n_ep), tp), device_id_type=MESH
        )

    sent = []

    def send(src, dst, device):
        copy = pltpu.make_async_remote_copy(
            src_ref=src,
            dst_ref=dst,
            send_sem=ssem.at[len(sent)],
            recv_sem=rsem.at[len(sent)],
            device_id=device,
            device_id_type=MESH,
        )
        copy.start()
        sent.append(copy)
        return copy

    peers = [(dh, dc) for dh in range(1, half) for dc in range(2)] + [(0, 1)]
    for i, (dh, dc) in enumerate(peers):
        part = matmul(gated_ref[...], outw_ref[:, columns(peer(dh, dc))])
        p_send[i] = part.astype(bf16)
    pl.semaphore_wait(barrier, n_tp + n_ep - 2)
    c_part = []
    for i, (dh, dc) in enumerate(peers):
        c_part.append(send(p_send.at[i], p_recv.at[i], (ep, peer(dh, dc))))
    c_sel = []
    for d in range(1, n_ep):
        target = lax.rem(ep + d, n_ep)
        c_sel.append(send(sel_ref.at[target], sel_recv.at[ep], (target, tp)))
    c_dense = [
        send(dg_hbm, wg.at[c], (ep, partner)),
        send(du_hbm, wu.at[c], (ep, partner)),
    ]
    sel_recv[ep] = sel_ref[ep]
    attended = matmul(gated_ref[...], outw_ref[:, own]).astype(bf16).astype(f32)
    for i in reversed(range(len(peers))):
        c_part[i].wait_recv()
        attended = attended + p_recv[i].astype(f32)
    middle = (hid_ref[:, own].astype(f32) + attended).astype(bf16).astype(f32)
    shaped = middle * gain_row[:, own]
    piece[ep] = shaped.astype(bf16)
    c_near = send(piece.at[ep], piece.at[ep], (near, tp))
    sides = [pl.ds(k * quarter // 2, quarter // 2) for k in range(2)]
    c_z = [None]
    for t in range(1, n_z):
        target = member(t, 0, ahead=True)
        c_z.append([send(piece.at[ep, :, k], piece.at[ep, :, k], (target, tp)) for k in sides])
    squares = jnp.sum(middle * middle, axis=-1, keepdims=True)
    inner = jnp.sum(shaped * gate_row[:, own], axis=-1, keepdims=True)
    line = lax.broadcasted_iota(jnp.int32, (tokens, lanes), 0)
    lane = lax.broadcasted_iota(jnp.int32, (tokens, lanes), 1)
    eye = jnp.where(line == lane, 1.0, 0.0)
    stat[tp, ep, 0:1, :] = jnp.sum(eye * squares, axis=0, keepdims=True)
    stat[tp, ep, 1:2, :] = jnp.sum(eye * inner, axis=0, keepdims=True)
    c_stat = []
    for d in range(1, n_ep):
        target = lax.rem(ep + d, n_ep)
        c_stat.append(send(stat.at[tp, ep], stat.at[tp, ep], (target, tp)))
    mid_buf[...] = middle

    c_other = {}

    def share(t, r):
        block = member(t, r)
        c_other[t, r] = send(piece.at[block], other.at[block], (ep, partner))

    def pick(q, t, r, source):
        block = member(t, r)
        picked = matmul(sel_recv[block][:, :tokens], source[block]).astype(bf16)
        rows_all[q, (2 * t + r) * cap : (2 * t + r + 1) * cap, :] = picked

    c_rows, c_pass, c_gu, c_hid, c_hid_near = {}, {}, {}, {}, {}
    c_eo_near, c_eo_far, c_y, c_out = {}, {}, {}, {}
    sub = tokens // half
    per_part = n_z // 2
    parts = [range(p * per_part, (p + 1) * per_part) for p in range(2)]

    def of_chip(value, index):
        chosen = value[:sub]
        for k in range(1, half):
            chosen = jnp.where(index == k, value[k * sub : (k + 1) * sub], chosen)
        return chosen

    def span_of(t):
        return pl.ds(2 * t * cap, 2 * cap)

    def send_rows(t):
        for dh in range(1, half):
            rows = rows_all.at[tp, span_of(t)]
            c_rows[t, dh] = send(rows, rows, (ep, peer(dh, 0)))

    def pass_rows(t):
        for dh in range(1, half):
            c_rows[t, dh].wait_recv()
            q = lax.rem(h - dh + half, half) * 2 + c
            rows = rows_all.at[q, span_of(t)]
            c_pass[t, dh] = send(rows, rows, (ep, partner))

    def partial(t):
        for r in range(2):
            c_other[t, r].wait_recv()
        block = jnp.where(c == 1, member(t, 1), member(t, 0))
        left, right = piece[block], other[block]
        for i, w in enumerate((wg, wu)):
            product = matmul(left, w[c]) + matmul(right, w[1 - c])
            gu_own[t, i] = of_chip(product, h)
            for dh in range(1, half):
                gu_send[t, dh - 1, i] = of_chip(product, lax.rem(h + dh, half)).astype(bf16)
        for dh in range(1, half):
            source, target = gu_send.at[t, dh - 1], gu_recv.at[t, dh - 1]
            c_gu[t, dh] = send(source, target, (ep, peer(dh, 0)))

    line_own = lax.broadcasted_iota(jnp.int32, (sub, lanes), 0) + h * sub
    eye_own = jnp.where(line_own == lax.broadcasted_iota(jnp.int32, (sub, lanes), 1), 1.0, 0.0)

    def activate(p):
        shares = []
        for t in parts[p]:
            gate_sum, up_sum = gu_own[t, 0], gu_own[t, 1]
            for dh in range(1, half):
                c_gu[t, dh].wait_recv()
                gate_sum = gate_sum + gu_recv[t, dh - 1, 0].astype(f32)
                up_sum = up_sum + gu_recv[t, dh - 1, 1].astype(f32)
            block = jnp.where(c == 1, member(t, 1), member(t, 0))
            scale = jnp.sum(eye_own * scale_rows[block, 0:1, :], axis=1, keepdims=True)
            shares.append(silu(gate_sum * scale) * (up_sum * scale))
        d_hid[tp, p] = jnp.concatenate(shares, axis=0).astype(bf16)
        mine = d_hid.at[tp, p]
        for dh in range(1, half):
            c_hid[p, dh] = send(mine, mine, (ep, peer(dh, 0)))
        c_hid_near[p, 0] = send(mine, mine, (ep, partner))

    def pass_hidden(p):
        for dh in range(1, half):
            c_hid[p, dh].wait_recv()
            got = d_hid.at[lax.rem(h - dh + half, half) * 2 + c, p]
            c_hid_near[p, dh] = send(got, got, (ep, partner))

    def dense_down(p):
        for dh in range(half):
            c_hid_near[p, dh].wait_recv()
        hidden = d_hid[:, p].reshape(n_tp * per_part * sub, units)
        d_out[p] = matmul(hidden, ddw[...]).reshape(d_out.shape[1:])

    def scales():
        for copy in c_total:
            copy.wait_recv()
        totals = stat[0]
        for q in range(1, n_tp):
            totals = totals + stat[q]
        factors = lax.rsqrt(totals[:, 0:1, :] / width + EPSILON)
        scale_rows[:, 0:1, :] = factors
        scale_rows[:, 1:2, :] = jax.nn.sigmoid(totals[:, 1:2, :] * factors)

    count = 2 * per_part * cap
    chosen_lane = lax.broadcasted_iota(jnp.int32, (cap, lanes), 1)

    def prepare(p):
        for t in parts[p]:
            for r in range(2):
                pick(partner, t, r, other)
                block = member(t, r)
                chosen = sel_recv[block].astype(f32)
                masked = jnp.where(chosen_lane < tokens, chosen * scale_rows[block, 0:1, :], 0.0)
                column = jnp.sum(masked, axis=1, keepdims=True)
                at = slice((2 * t + r) * cap, (2 * t + r + 1) * cap)
                row_scale[at, :] = jnp.broadcast_to(column, (cap, lanes))

    inner_width = eg.shape[1]
    tile = 256 if inner_width % 256 == 0 else 128

    def expert_in(p):
        for t in parts[p]:
            for dh in range(1, half):
                c_pass[t, dh].wait_recv()
        at = slice(p * count, (p + 1) * count)

        scale = row_scale[at, 0:1]
        for i in range(inner_width // tile):
            cols = slice(i * tile, (i + 1) * tile)
            gate_part = matmul(rows_all[0, at], eg[0:quarter, cols])
            up_part = matmul(rows_all[0, at], eu[0:quarter, cols])
            for q in range(1, n_tp):
                span = slice(q * quarter, (q + 1) * quarter)
                gate_part = gate_part + matmul(rows_all[q, at], eg[span, cols])
                up_part = up_part + matmul(rows_all[q, at], eu[span, cols])
            e_hid[at, cols] = (silu(gate_part * scale) * (up_part * scale)).astype(bf16)

    def expert_near(p):
        at = slice(p * count, (p + 1) * count)
        for i, dh in enumerate(list(range(1, half)) + [0]):
            near_send[p, i] = matmul(e_hid[at, :], ed[:, columns(peer(dh, 1))]).astype(bf16)
            source, target = near_send.at[p, i], near_recv.at[p, i]
            c_eo_near[p, i] = send(source, target, (ep, partner))

    def far_first(p):
        return [t for t in parts[p] if t] + [t for t in parts[p] if not t]

    def expert_far(p):
        at = slice(p * count, (p + 1) * count)
        for i, dh in enumerate(range(1, half)):
            part = matmul(e_hid[at, :], ed[:, columns(peer(dh, 0))])
            c_eo_near[p, i].wait_recv()
            far_send[p, i] = (part + near_recv[p, i].astype(f32)).astype(bf16)
            for t in far_first(p):
                rows = pl.ds(2 * (t % per_part) * cap, 2 * cap)
                source, target = far_send.at[p, i, rows], far_recv.at[p, i, rows]
                c_eo_far[t, i] = send(source, target, (ep, peer(dh, 0)))

    def expert_own(p):
        at = slice(p * count, (p + 1) * count)
        part = matmul(e_hid[at, :], ed[:, own])
        c_eo_near[p, half - 1].wait_recv()
        eo_own[at, :] = part + near_recv[p, half - 1].astype(f32)

    def expert_total(t):
        at = slice(2 * t * cap, 2 * (t + 1) * cap)
        p, k = t // per_part, t % per_part
        total = eo_own[at, :]
        for i in range(half - 1):
            c_eo_far[t, i].wait_recv()
            total = total + far_recv[p, i, 2 * k * cap : 2 * (k + 1) * cap].astype(f32)
        eo_own[at, :] = total

    def outcome(t, r):
        block = member(t, r)
        span = slice((2 * t + r) * cap, (2 * t + r + 1) * cap)
        chosen = sel_recv[block]
        weight = chosen[:, lanes - 2 : lanes - 1].astype(f32)
        weight = weight + chosen[:, lanes - 1 : lanes].astype(f32)
        answers = (eo_own[span, :] * weight).astype(bf16)
        routed = lax.dot_general(
            chosen[:, :tokens], answers, (((0,), (0,)), ((), ())), preferred_element_type=f32
        )
        branch = jnp.sum(eye * scale_rows[block, 1:2, :], axis=1, keepdims=True)
        p, k = t // per_part, t % per_part
        dense = [d_out[p, 2 * j + r, k * sub : (k + 1) * sub, :] for j in range(half)]
        return branch * jnp.concatenate(dense, axis=0) + routed

    halves = [slice(k * quarter // 2, (k + 1) * quarter // 2) for k in range(2)]

    def send_near(p):
        for t in far_first(p):
            expert_total(t)
            mine = outcome(t, 1).astype(bf16)
            for k in range(2):
                y_send[t, k] = mine[:, halves[k]]
                c_y[t, k] = send(y_send.at[t, k], y_recv.at[t, k], (near, tp))

    def send_out(ts):
        for t in ts:
            mine = outcome(t, 0)
            for k in range(2):
                c_y[t, k].wait_recv()
                total = mine[:, halves[k]] + y_recv[t, k].astype(f32)
                if t:
                    z_send[t - 1, k] = total.astype(bf16)
                    source, target = z_send.at[t - 1, k], z_recv.at[t - 1, k]
                    c_out[t, k] = send(source, target, (member(t, 0), tp))
                else:
                    mid_buf[:, halves[k]] = mid_buf[:, halves[k]] + total

    share(0, 0)
    for copy in c_sel:
        copy.wait_recv()
    pick(tp, 0, 0, piece)
    c_near.wait_recv()
    share(0, 1)
    pick(tp, 0, 1, piece)
    send_rows(0)
    c_relay = [None]
    for t in range(1, n_z):
        block = member(t, 0)
        c_relay.append([])
        for copy, k in zip(c_z[t], sides):
            copy.wait_recv()
            c_relay[t].append(send(piece.at[block, :, k], piece.at[block, :, k], (near, tp)))
        share(t, 0)
        pick(tp, t, 0, piece)
        if t == 1:
            loads[0].wait()
            loads[1].wait()
            for copy in c_dense:
                copy.wait_recv()
            partial(0)
    c_total = []
    for t in range(1, n_z):
        for copy in c_relay[t]:
            copy.wait_recv()
        share(t, 1)
        pick(tp, t, 1, piece)
        send_rows(t)
        if t == 1:
            for copy in c_stat:
                copy.wait_recv()
            for dh, dc in peers:
                c_total.append(send(stat.at[tp], stat.at[tp], (ep, peer(dh, dc))))
        if t > 1:
            partial(t - 1)
        if t != 2:
            pass_rows(max(t - 2, 0))
    partial(n_z - 1)
    scales()
    prepare(0)
    for t in range(max(n_z - 2, 1), per_part):
        pass_rows(t)
    loads[2].wait()
    loads[3].wait()
    expert_in(0)
    loads[4].wait()
    expert_near(0)
    for t in range(max(n_z - 2, per_part), n_z):
        pass_rows(t)
    activate(0)
    prepare(1)
    expert_far(0)
    activate(1)
    expert_in(1)
    expert_near(1)
    pass_hidden(0)
    expert_own(0)
    expert_far(1)
    pass_hidden(1)
    expert_own(1)
    loads[5].wait()
    dense_down(0)
    send_near(0)
    dense_down(1)
    send_near(1)
    send_out(range(1, per_part))
    send_out(range(per_part, n_z))
    send_out([0])
    for k in range(2):
        mine = mid_buf[:, halves[k]]
        for t in range(1, n_z):
            c_out[t, k].wait_recv()
            mine = mine + z_recv[t - 1, k].astype(f32)
        mixed_ref[:, halves[k]] = mine.astype(bf16)
    for copy in sent:
        copy.wait_send()


def run_layer(gated, output_weight, hid, gain, gate, sel, eg, eu, ed, dg, du, dd):
    n_ep, n_tp = lax.axis_size("ep"), lax.axis_size("tp")
    tokens = hid.shape[0]
    quarter = hid.shape[1] // n_tp
    cap, lanes = sel.shape[1:]
    items = n_ep * cap
    n_z, half = n_ep // 2, n_tp // 2
    sub = tokens // half
    part = items // 2
    units = dg.shape[1]
    bf16, f32 = jnp.bfloat16, jnp.float32
    vmem = pl.BlockSpec(memory_space=pltpu.VMEM)
    anyspace = pl.BlockSpec(memory_space=pl.ANY)
    copies = 8 * n_ep + 4 * n_tp + 12 * n_z + 16
    scratch = [pltpu.VMEM(w.shape, bf16) for w in (eg, eu, ed)]
    scratch += [
        pltpu.VMEM((2, quarter, units), bf16),
        pltpu.VMEM((2, quarter, units), bf16),
        pltpu.VMEM(dd.shape, bf16),
        pltpu.VMEM((1, hid.shape[1]), f32),
        pltpu.VMEM((1, hid.shape[1]), f32),
        pltpu.VMEM(sel.shape, bf16),
        pltpu.VMEM((n_tp - 1, tokens, quarter), bf16),
        pltpu.VMEM((n_tp - 1, tokens, quarter), bf16),
        pltpu.VMEM((n_tp, n_ep, 2, lanes), f32),
        pltpu.VMEM((n_ep, 2, lanes), f32),
        pltpu.VMEM((tokens, quarter), f32),
        pltpu.VMEM((n_ep, tokens, quarter), bf16),
        pltpu.VMEM((n_ep, tokens, quarter), bf16),
        pltpu.VMEM((n_tp, items, quarter), bf16),
        pltpu.VMEM((items, lanes), f32),
        pltpu.VMEM((n_z, half - 1, 2, sub, units), bf16),
        pltpu.VMEM((n_z, half - 1, 2, sub, units), bf16),
        pltpu.VMEM((n_z, 2, sub, units), f32),
        pltpu.VMEM((items, eg.shape[1]), bf16),
        pltpu.VMEM((2, half, part, quarter), bf16),
        pltpu.VMEM((2, half, part, quarter), bf16),
        pltpu.VMEM((2, half - 1, part, quarter), bf16),
        pltpu.VMEM((2, half - 1, part, quarter), bf16),
        pltpu.VMEM((items, quarter), f32),
        pltpu.VMEM((n_tp, 2, n_z // 2 * sub, units), bf16),
        pltpu.VMEM((2, n_tp, n_z // 2 * sub, quarter), f32),
        pltpu.VMEM((n_z, 2, tokens, quarter // 2), bf16),
        pltpu.VMEM((n_z, 2, tokens, quarter // 2), bf16),
        pltpu.VMEM((n_z - 1, 2, tokens, quarter // 2), bf16),
        pltpu.VMEM((n_z - 1, 2, tokens, quarter // 2), bf16),
        pltpu.SemaphoreType.DMA((6,)),
        pltpu.SemaphoreType.DMA((copies,)),
        pltpu.SemaphoreType.DMA((copies,)),
    ]
    return pl.pallas_call(
        functools.partial(layer_kernel, n_ep, n_tp),
        out_shape=jax.ShapeDtypeStruct((tokens, quarter), bf16),
        in_specs=[vmem] * 6 + [anyspace] * 6,
        out_specs=vmem,
        scratch_shapes=scratch,
        compiler_params=pltpu.CompilerParams(
            collective_id=0, has_side_effects=True, vmem_limit_bytes=36 * 1024 * 1024
        ),
    )(gated, output_weight, hid, gain, gate, sel, *map(in_hbm, (eg, eu, ed, dg, du, dd)))


def attention_kernel(
    cap,
    hidden_hbm,
    gain_hbm,
    shift_hbm,
    head_gain_hbm,
    routes_hbm,
    weights_hbm,
    qw_hbm,
    kw_hbm,
    vw_hbm,
    ow_hbm,
    fw_hbm,
    state_hbm,
    outw_hbm,
    gated_ref,
    sel_ref,
    hidden_ref,
    outw_ref,
    new_hbm,
    gain_ref,
    shift_ref,
    head_gain_ref,
    routes_ref,
    weights_ref,
    qw,
    kw,
    vw,
    ow,
    fw,
    state,
    key_query,
    value,
    decay,
    readout,
    w_sem,
    in_sem,
    out_sem,
):
    f32, bf16 = jnp.float32, jnp.bfloat16
    tokens = hidden_hbm.shape[0]
    heads, key_dim, value_dim = state.shape[1:]
    groups = tokens // 8
    loads = []
    pairs = (
        (fw_hbm, fw),
        (kw_hbm, kw),
        (qw_hbm, qw),
        (vw_hbm, vw),
        (ow_hbm, ow),
        (hidden_hbm, hidden_ref),
        (gain_hbm, gain_ref),
        (routes_hbm, routes_ref),
        (weights_hbm, weights_ref),
        (shift_hbm, shift_ref),
        (head_gain_hbm, head_gain_ref),
        (outw_hbm, outw_ref),
    )
    for i, (src, dst) in enumerate(pairs):
        loads.append(pltpu.make_async_copy(src, dst, w_sem.at[i]))
    for i in (5, 6, 7, 8, 0, 1, 2, 3, 9, 10):
        loads[i].start()

    def fetch(g):
        rows = pl.ds(g * 8, 8)
        return pltpu.make_async_copy(state_hbm.at[rows], state.at[rows], in_sem.at[g])

    def put(g):
        rows = pl.ds(g * 8, 8)
        return pltpu.make_async_copy(state.at[rows], new_hbm.at[rows], out_sem.at[g])

    loads[5].wait()
    for g in range(groups):
        fetch(g).start()
    loads[4].start()
    loads[11].start()
    loads[6].wait()
    inputs = hidden_ref[...].astype(f32)
    normed = (inputs * rms_factor(inputs) * flat_row(gain_ref)).astype(bf16)

    loads[7].wait()
    loads[8].wait()
    items, lanes = sel_ref.shape
    experts = (items // cap + 7) // 8 * 8
    first, second = routes_ref[0:1, :], routes_ref[1:2, :]
    expert = lax.broadcasted_iota(jnp.int32, (experts, tokens), 0)
    chosen0 = jnp.where(expert == first, 1.0, 0.0)
    chosen1 = jnp.where(expert == second, 1.0, 0.0)
    row = lax.broadcasted_iota(jnp.int32, (tokens, tokens), 0)
    col = lax.broadcasted_iota(jnp.int32, (tokens, tokens), 1)
    before = jnp.where(row < col, 1.0, 0.0).astype(bf16)
    earlier = matmul((chosen0 + chosen1).astype(bf16), before)
    slot0 = jnp.sum(earlier * chosen0, axis=0, keepdims=True)
    slot1 = jnp.sum(earlier * chosen1, axis=0, keepdims=True)
    table = lax.broadcasted_iota(jnp.int32, (items, tokens), 0)
    hit0 = table == first * cap + slot0.astype(jnp.int32)
    hit1 = table == second * cap + slot1.astype(jnp.int32)
    comb = jnp.where(hit0, weights_ref[0:1, :], 0.0) + jnp.where(hit1, weights_ref[1:2, :], 0.0)
    weight = jnp.sum(comb, axis=1, keepdims=True)
    weight_hi = weight.astype(bf16).astype(f32)
    lane = lax.broadcasted_iota(jnp.int32, (items, lanes), 1)
    tail = jnp.where(lane == lanes - 2, weight_hi, weight - weight_hi)
    sel_ref[...] = jnp.where(lane < lanes - 2, 0.0, tail).astype(bf16)
    sel_ref[:, :tokens] = (jnp.where(hit0, 1.0, 0.0) + jnp.where(hit1, 1.0, 0.0)).astype(bf16)

    def rounded_rows(weight):
        return matmul(normed, weight[...]).astype(bf16).astype(f32)

    loads[0].wait()
    loads[9].wait()
    loads[10].wait()
    drive = matmul(normed, fw[...])
    log_sig = jnp.minimum(drive, 0.0) - jnp.log1p(jnp.exp(-jnp.abs(drive)))
    decay[...] = jnp.exp(log_sig / TAU_DECAY + shift_ref[...]).reshape(decay.shape)
    loads[1].wait()
    key_query[:, 0:8] = rounded_rows(kw).reshape(decay.shape)
    loads[2].wait()
    key_query[:, 8:16] = rounded_rows(qw).reshape(decay.shape)
    loads[3].wait()
    value[...] = rounded_rows(vw).reshape(value.shape)
    spread_width = value_dim + 128
    token = lax.broadcasted_iota(jnp.int32, (16, spread_width), 0)
    column = lax.broadcasted_iota(jnp.int32, (16, spread_width), 1)
    unit = jnp.ones((1, 128), f32)

    @pl.loop(0, groups)
    def _(g):
        fetch(g).wait()
        for h in range(heads):
            keys = slice(h * key_dim, (h + 1) * key_dim)
            vals = slice(h * value_dim, (h + 1) * value_dim)
            decay_cols = jnp.transpose(decay[g, :, keys])
            left = jnp.transpose(key_query[g, :, keys]).astype(bf16)
            for j in range(8):
                right = jnp.concatenate([value[g, j : j + 1, vals], unit], axis=1)
                wanted = token == jnp.where(column < value_dim, j, 8 + j)
                products = matmul(left, jnp.where(wanted, right, 0.0).astype(bf16))
                fresh = decay_cols[:, j : j + 1] * state[g * 8 + j, h] + products[:, :value_dim]
                state[g * 8 + j, h] = fresh
                asked = products[:, value_dim:]
                asked = jnp.concatenate([asked] * (value_dim // 128), axis=1)
                readout[g, j : j + 1, vals] = jnp.sum(asked * fresh, axis=0, keepdims=True)
        put(g).start()

    loads[4].wait()
    outgate = rounded_rows(ow)
    out = readout[...].reshape(tokens, heads * value_dim) * key_dim ** (-0.5)
    for h in range(heads):
        vals = slice(h * value_dim, (h + 1) * value_dim)
        part = out[:, vals]
        gain = head_gain_ref[:, vals].astype(f32)
        gated_ref[:, vals] = (part * rms_factor(part) * gain * silu(outgate[:, vals])).astype(bf16)
    loads[11].wait()
    for g in range(groups):
        put(g).wait()


def run_attention(
    hidden, gain, shift, head_gain, routes, weights, qw, kw, vw, ow, fw, state, outw, n_ep
):
    bf16, f32 = jnp.bfloat16, jnp.float32
    tokens, heads, key_dim, value_dim = state.shape
    capacity = tokens * routes.shape[0] // n_ep + 2
    cap = (capacity + 15) // 16 * 16
    items = n_ep * cap
    groups = tokens // 8
    lanes = (tokens + 2 + 127) // 128 * 128
    vmem = pl.BlockSpec(memory_space=pltpu.VMEM)
    anyspace = pl.BlockSpec(memory_space=pl.ANY)
    operands = (hidden, gain, shift, head_gain, routes, weights, qw, kw, vw, ow, fw, state, outw)
    gated, sel, hidden, outw, new_state = pl.pallas_call(
        functools.partial(attention_kernel, cap),
        out_shape=(
            pltpu.VMEM((tokens, heads * value_dim), bf16),
            pltpu.VMEM((items, lanes), bf16),
            pltpu.VMEM(hidden.shape, bf16),
            pltpu.VMEM(outw.shape, bf16),
            jax.ShapeDtypeStruct(state.shape, f32),
        ),
        in_specs=[anyspace] * 13,
        out_specs=(vmem, vmem, vmem, vmem, anyspace),
        scratch_shapes=[pltpu.VMEM(a.shape, a.dtype) for a in operands[1:11]]
        + [
            pltpu.VMEM(state.shape, f32),
            pltpu.VMEM((groups, 16, heads * key_dim), f32),
            pltpu.VMEM((groups, 8, heads * value_dim), f32),
            pltpu.VMEM((groups, 8, heads * key_dim), f32),
            pltpu.VMEM((groups, 8, heads * value_dim), f32),
            pltpu.SemaphoreType.DMA((12,)),
            pltpu.SemaphoreType.DMA((groups,)),
            pltpu.SemaphoreType.DMA((groups,)),
        ],
        compiler_params=pltpu.CompilerParams(vmem_limit_bytes=24 * 1024 * 1024),
    )(*map(in_hbm, operands))
    return gated, sel.reshape(n_ep, cap, lanes), hidden, outw, new_state


def body(
    hidden_in,
    carried_state,
    input_gain,
    query_weight,
    key_weight,
    value_weight,
    outgate_weight,
    decay_weight,
    decay_shift,
    head_gain,
    output_weight,
    channel_gain,
    branch_gate,
    routes,
    route_weights,
    expert_gate,
    expert_up,
    expert_down,
    dense_gate,
    dense_up,
    dense_down,
):
    gated, sel, hidden, outw, new_state = run_attention(
        hidden_in,
        input_gain.reshape(-1, 128),
        decay_shift,
        head_gain.reshape(1, -1),
        routes.T,
        route_weights.T,
        query_weight,
        key_weight,
        value_weight,
        outgate_weight,
        decay_weight,
        carried_state,
        output_weight,
        lax.axis_size("ep"),
    )
    mixed = run_layer(
        gated,
        outw,
        hidden,
        channel_gain.reshape(-1, 128),
        branch_gate.reshape(-1, 128),
        sel,
        expert_gate[0],
        expert_up[0],
        expert_down[0],
        dense_gate,
        dense_up,
        dense_down,
    )
    return (mixed, new_state)


def solution(mesh):
    in_specs = (
        P("ep", None),
        P("ep", "tp", None, None),
        P(),
        P(None, "tp"),
        P(None, "tp"),
        P(None, "tp"),
        P(None, "tp"),
        P(None, "tp"),
        P("ep", "tp"),
        P("tp", None),
        P("tp", None),
        P(),
        P(),
        P("ep", None),
        P("ep", None),
        P("ep", None, "tp"),
        P("ep", None, "tp"),
        P("ep", "tp", None),
        P("tp", "ep"),
        P("tp", "ep"),
        P("ep", "tp"),
    )
    out_specs = (P("ep", "tp"), P("ep", "tp", None, None))
    return jax.shard_map(body, mesh=mesh, in_specs=in_specs, out_specs=out_specs, check_vma=False)
```
